256 devices in a mesh: kv: 32 (over z, y), tp: 8 (over x, core).
Axes of the slice: x: 4, y: 4, z: 8, core: 2. Of those that a mesh axis runs over, the one named last changes fastest.
Arguments:
- tokens: bfloat16 [16, 4096], P(None, ('kv', 'tp')), may hold values from -17 to 17
- first_gain: float32 [4096], P('kv'), may hold values from 0.1 to 1.9
- first_gate: bfloat16 [4096, 11264], P('kv', 'tp'), may hold values from -0.09375 to 0.09375
- first_up: bfloat16 [4096, 11264], P('kv', 'tp'), may hold values from -0.09375 to 0.09375
- first_down: bfloat16 [11264, 4096], P('tp', 'kv'), may hold values from -0.0546875 to 0.0546875
- mixer_gain: float32 [4096], P('kv'), may hold values from 0.1 to 1.9
- w_query: bfloat16 [4096, 4096], P('kv', 'tp'), may hold values from -0.09375 to 0.09375
- w_key: bfloat16 [4096, 4096], P('kv', 'tp'), may hold values from -0.328125 to 0.328125
- w_value: bfloat16 [4096, 4096], P('kv', 'tp'), may hold values from -0.09375 to 0.09375
- w_output: bfloat16 [4096, 4096], P('tp', 'kv'), may hold values from -0.09375 to 0.09375
- lam_heads: float32 [32], P('tp'), may hold values from 0.3 to 0.8
- head_gain: float32 [128], replicated, may hold values from 0.1 to 1.9
- key_cache: bfloat16 [16, 8192, 32, 128], P(None, 'kv', 'tp'), may hold values from -1000 to 1000
- value_cache: bfloat16 [16, 8192, 32, 128], P(None, 'kv', 'tp'), may hold values from -6 to 6
- lengths: int32 [16], replicated, may hold values from 1 to 8192, 49152 in all
- last_gain: float32 [4096], P('kv'), may hold values from 0.1 to 1.9
- last_gate: bfloat16 [4096, 11264], P('kv', 'tp'), may hold values from -0.09375 to 0.09375
- last_up: bfloat16 [4096, 11264], P('kv', 'tp'), may hold values from -0.09375 to 0.09375
- last_down: bfloat16 [11264, 4096], P('tp', 'kv'), may hold values from -0.0546875 to 0.0546875
Outputs:
- result: bfloat16 [16, 4096], P(None, ('kv', 'tp'))
The draws below stay inside these ranges and needn't reach their ends.
Inputs may be any that keep to these rules, and one draw needn't show every extreme that they name: Sequence b reads cached positions 0 to lengths[b] - 1 and its new token.
All inputs are finite; a program needn't handle non-finite values.
Results may differ from the reference program's by a relative error of at most 0.04.
Values may be sent and summed in bfloat16 or wider, within the bound.
No kernel may reach another device: no remote copies, remote signals or barrier semaphores. Data moves between devices by JAX's collectives and lax.ppermute only.
A program may use at most 64 MiB of HBM per device.

```python
import math
import jax
import jax.numpy as jnp
import numpy as np
from jax import lax

WIDTH = 4096
HEADS = 32
HEAD_DIM = 64
VAL_DIM = 128
FFN_UNITS = 11264
BATCH = 16
SEQ_LEN = 8192


def draw_tokens(key, part):
    base = jnp.clip(jax.random.normal(jax.random.fold_in(key, 11), (BATCH, WIDTH), jnp.float32), -6.0, 6.0)
    column = jnp.arange(WIDTH, dtype=jnp.float32) / (WIDTH - 1)
    logit_scale = 0.6 * jnp.exp(jnp.log(4.0) * column)[None, :]
    return (base * logit_scale).astype(jnp.bfloat16)


def draw_key_cache(key, part):
    shape = (BATCH, SEQ_LEN, HEADS, 2 * HEAD_DIM)
    base = 1.75 * jnp.clip(jax.random.normal(jax.random.fold_in(key, 21), shape, jnp.float32), -8.0, 8.0)
    return base.astype(jnp.bfloat16)


def block_levels(rng, dims, split, low, top_value):
    def one(axis_at, parts):
        steps = jax.random.uniform(jax.random.fold_in(jax.random.fold_in(rng, 6), axis_at), (parts,), jnp.float32, low / len(split), top_value / len(split))
        return jnp.repeat(jnp.exp(steps), dims[axis_at] // parts).reshape((-1,) + (1,) * (len(dims) - axis_at - 1))

    loudness = one(*split[0])
    for cut in split[1:]:
        loudness = loudness * one(*cut)
    return loudness


def length_profile(count, total, reach, slope):
    weights = [(1 << 20) // math.isqrt(standing ** slope) + 1 for standing in range(2, count + 1)]
    spare, counts = total - reach - (count - 1), [1] * (count - 1)
    while spare > 0:
        movable = [i for i in range(count - 1) if counts[i] < reach]
        mass, budget = sum([weights[i] for i in movable]), spare
        for i in movable:
            addition = min(reach - counts[i], max(1, budget * weights[i] // mass), spare)
            counts[i] = counts[i] + addition
            spare = spare - addition
    return np.array([reach] + counts)


def uneven_parts(key, amount, total, bound, slope):
    if amount == 2:
        one = jax.random.randint(key, (), max(1, total - bound), min(bound, total - 1) + 1)
        return jnp.stack([one, total - one])
    sizes = jnp.asarray(length_profile(amount, total, bound, slope), jnp.int32)
    pairs = (amount - 1) // 2
    giver, sink = sizes[1:1 + 2 * pairs:2], sizes[2:2 + 2 * pairs:2]
    slack = jnp.minimum(giver - 1, bound - sink)
    moved = jax.random.randint(jax.random.fold_in(key, 1), (pairs,), 0, 1 << 20) % (slack + 1)
    sizes = sizes.at[1:1 + 2 * pairs:2].set(giver - moved).at[2:2 + 2 * pairs:2].set(sink + moved)
    return sizes[jax.random.permutation(jax.random.fold_in(key, 2), amount)]


def noise(key, shape, deviation, limit, cuts=(), kind=jnp.bfloat16):
    result = deviation * jax.random.normal(key, shape, jnp.float32)
    if cuts:
        result = result * block_levels(key, shape, cuts, -0.22, 0.18)
    return jnp.clip(result, -limit, limit).astype(kind)


def setup_inputs(seed: int = 0) -> dict:
    streams_of = jax.random.split(jax.random.key(seed), 20)
    return {
        "tokens": draw_tokens(jax.random.fold_in(streams_of[19], 71), 0),
        "first_gain": jnp.clip(1.0 + 0.18 * jax.random.normal(streams_of[1], (WIDTH,), jnp.float32), 0.1, 1.9),
        "first_gate": noise(streams_of[2], (WIDTH, FFN_UNITS), WIDTH ** -0.5, 0.09375, ((0, 32), (1, 8))),
        "first_up": noise(streams_of[3], (WIDTH, FFN_UNITS), WIDTH ** -0.5, 0.09375, ((0, 32), (1, 8))),
        "first_down": noise(streams_of[4], (FFN_UNITS, WIDTH), FFN_UNITS ** -0.5, 0.0546875, ((0, 8), (1, 32))),
        "mixer_gain": jnp.clip(1.0 + 0.18 * jax.random.normal(streams_of[5], (WIDTH,), jnp.float32), 0.1, 1.9),
        "w_query": noise(streams_of[6], (WIDTH, HEADS * 2 * HEAD_DIM), WIDTH ** -0.5, 0.09375, ((0, 32), (1, 8))),
        "w_key": noise(streams_of[7], (WIDTH, HEADS * 2 * HEAD_DIM), (3.5 / WIDTH ** 0.5), 0.328125, ((0, 32), (1, 8))),
        "w_value": noise(streams_of[8], (WIDTH, HEADS * VAL_DIM), WIDTH ** -0.5, 0.09375, ((0, 32), (1, 8))),
        "w_output": noise(streams_of[9], (HEADS * VAL_DIM, WIDTH), (HEADS * VAL_DIM) ** -0.5, 0.09375, ((0, 8), (1, 32))),
        "lam_heads": jnp.clip(0.3 + 0.5 * jax.random.uniform(streams_of[10], (HEADS,), jnp.float32) ** block_levels(streams_of[10], (HEADS,), ((0, 8),), -0.2, 0.2), 0.3, 0.8),
        "head_gain": jnp.clip(1.0 + 0.18 * jax.random.normal(streams_of[11], (VAL_DIM,), jnp.float32), 0.1, 1.9),
        "key_cache": draw_key_cache(jax.random.fold_in(streams_of[19], 71), 0),
        "value_cache": noise(streams_of[13], (BATCH, SEQ_LEN, HEADS, VAL_DIM), 1.0, 6.0, ((1, 32), (2, 8))),
        "lengths": uneven_parts(streams_of[14], BATCH, 3 * SEQ_LEN * BATCH // 8, SEQ_LEN, 2).astype(jnp.int32),
        "last_gain": jnp.clip(1.0 + 0.18 * jax.random.normal(streams_of[15], (WIDTH,), jnp.float32), 0.1, 1.9),
        "last_gate": noise(streams_of[16], (WIDTH, FFN_UNITS), WIDTH ** -0.5, 0.09375, ((0, 32), (1, 8))),
        "last_up": noise(streams_of[17], (WIDTH, FFN_UNITS), WIDTH ** -0.5, 0.09375, ((0, 32), (1, 8))),
        "last_down": noise(streams_of[18], (FFN_UNITS, WIDTH), FFN_UNITS ** -0.5, 0.0546875, ((0, 8), (1, 32))),
    }


epsilon = 1e-06
neg_fill = -1e+30

def gated_units(stream, gain, gate_w, up_w, down_w):
    wide = stream.astype(jnp.float32)
    inv_rms = lax.rsqrt(lax.optimization_barrier(jnp.mean(wide * wide, axis=1, keepdims=True)) + epsilon)
    scaled = (wide * gain).astype(jnp.bfloat16)
    gate_pre = jnp.dot(scaled, gate_w, preferred_element_type=jnp.float32) * inv_rms
    up_pre = jnp.dot(scaled, up_w, preferred_element_type=jnp.float32) * inv_rms
    hidden_act = (jax.nn.silu(gate_pre) * up_pre).astype(jnp.bfloat16)
    return jnp.dot(hidden_act, down_w, preferred_element_type=jnp.float32)

def one_sequence(items):
    query_rows, keys, values, length, fresh_key, new_value, lam_heads = items
    seq_len = keys.shape[0]
    logit_scale = HEAD_DIM ** (-0.5)
    query_single32 = query_rows.astype(jnp.float32)
    key_entries = keys.astype(jnp.float32).reshape(seq_len, HEADS, 2, HEAD_DIM)
    score_matrix = jnp.einsum('fuz,tfuz->fut', query_single32, key_entries) * logit_scale
    positions = jnp.arange(seq_len, dtype=jnp.int32)
    live_mask = (positions < length)[None, None, :]
    score_matrix = jnp.where(live_mask, score_matrix, neg_fill)
    self_score = jnp.einsum('vij,vij->vi', query_single32, fresh_key.astype(jnp.float32)) * logit_scale
    highest = jnp.maximum(lax.optimization_barrier(jnp.max(score_matrix, axis=-1)), self_score)
    weights = jnp.where(live_mask, jnp.exp(score_matrix - highest[..., None]), 0.0)
    own_weight = jnp.exp(self_score - highest)
    totals = lax.optimization_barrier(jnp.sum(weights, axis=-1)) + own_weight
    rounded = lax.optimization_barrier(weights.astype(jnp.bfloat16)).astype(jnp.float32)
    own_round = lax.optimization_barrier(own_weight.astype(jnp.bfloat16)).astype(jnp.float32)
    weighted = jnp.einsum('hml,lhe->hme', rounded, values.astype(jnp.float32))
    weighted = weighted + own_round[..., None] * new_value.astype(jnp.float32)[:, None, :]
    return weighted[:, 0] / totals[:, 0, None] - lam_heads[:, None] * weighted[:, 1] / totals[:, 1, None]

def reference(tokens, first_gain, first_gate, first_up, first_down, mixer_gain, w_query, w_key, w_value, w_output, lam_heads, head_gain, key_cache, value_cache, lengths, last_gain, last_gate, last_up, last_down):
    batch = tokens.shape[0]
    first = (tokens.astype(jnp.float32) + 0.5 * gated_units(tokens, first_gain, first_gate, first_up, first_down)).astype(jnp.bfloat16)
    wide = first.astype(jnp.float32)
    inv_rms = lax.rsqrt(lax.optimization_barrier(jnp.mean(wide * wide, axis=1, keepdims=True)) + epsilon)
    scaled = (wide * mixer_gain).astype(jnp.bfloat16)
    query_rows = (jnp.dot(scaled, w_query, preferred_element_type=jnp.float32) * inv_rms).astype(jnp.bfloat16)
    fresh_key = (jnp.dot(scaled, w_key, preferred_element_type=jnp.float32) * inv_rms).astype(jnp.bfloat16)
    new_value = (jnp.dot(scaled, w_value, preferred_element_type=jnp.float32) * inv_rms).astype(jnp.bfloat16)
    query_rows = query_rows.reshape(batch, HEADS, 2, HEAD_DIM)
    fresh_key = fresh_key.reshape(batch, HEADS, 2, HEAD_DIM)
    new_value = new_value.reshape(batch, HEADS, VAL_DIM)
    lam_rows = jnp.broadcast_to(lam_heads, (batch, HEADS))
    mixed = lax.map(one_sequence, (query_rows, key_cache, value_cache, lengths, fresh_key, new_value, lam_rows))
    normed = mixed * lax.rsqrt(lax.optimization_barrier(jnp.mean(mixed * mixed, axis=-1, keepdims=True)) + epsilon) * head_gain
    attended = normed.astype(jnp.bfloat16).reshape(batch, HEADS * VAL_DIM)
    projected = jnp.dot(attended, w_output, preferred_element_type=jnp.float32)
    second = (wide + projected).astype(jnp.bfloat16)
    last = gated_units(second, last_gain, last_gate, last_up, last_down)
    return (second.astype(jnp.float32) + 0.5 * last).astype(jnp.bfloat16)
```

```python
import functools

import jax
import jax.numpy as jnp
from jax import lax
from jax.experimental import pallas as pl
from jax.experimental.pallas import tpu as pltpu
from jax.sharding import Mesh
from jax.sharding import PartitionSpec as P

WIDTH = 4096
ROWS = 16
HEAD_DIM = 64
LANES = 128
KV = ("kv_0", "kv_1")
KV_TP = ("kv_0", "kv_1", "tp")

epsilon = 1e-06
neg_fill = -1e30
f32 = jnp.float32
bf16 = jnp.bfloat16


def iota(shape, dim):
    return lax.broadcasted_iota(jnp.int32, shape, dim)


def matmul(a, b):
    return jnp.dot(a, b, preferred_element_type=f32)


def in_kernel(body, outs, *args, smem=(), vmem_limit=16 << 20):
    spaces = [pltpu.SMEM if k in smem else pltpu.VMEM for k in range(len(args))]
    return pl.pallas_call(
        body,
        out_shape=outs,
        in_specs=[pl.BlockSpec(memory_space=space) for space in spaces],
        out_specs=jax.tree.map(lambda _: pl.BlockSpec(memory_space=pltpu.VMEM), outs),
        compiler_params=pltpu.CompilerParams(vmem_limit_bytes=vmem_limit),
        name=body.__name__,
    )(*args)


def swap(blocks, axis):
    return lax.all_to_all(blocks, axis, split_axis=0, concat_axis=0, tiled=True)


def like(shape, kind):
    return jax.ShapeDtypeStruct(shape, kind)


def kv_index():
    return lax.axis_index("kv_0") * lax.axis_size("kv_1") + lax.axis_index("kv_1")


def halves(column):
    high = column.astype(bf16)
    low = (column - high.astype(f32)).astype(bf16)
    return high.astype(f32), low.astype(f32)


def thirds(column):
    high, low = halves(column)
    rest = (column - high) - low
    return high, low, rest


def own_columns(shape_dim):
    place = lax.axis_index("tp") * ROWS
    return (iota((ROWS, LANES), 1) == iota((ROWS, LANES), 0) + place).astype(bf16)


def spread_tokens(tokens_ref, out_ref):
    block = matmul(tokens_ref[...], own_columns(0)).astype(bf16)
    out_ref[...] = jnp.broadcast_to(block[None], out_ref.shape)


def send_units(stream, gain_ref, gate_ref, up_ref, out_ref):
    wide = stream.astype(f32)
    high, low = halves(jnp.sum(wide * wide, axis=1, keepdims=True))
    scaled = (wide * gain_ref[...]).astype(bf16)
    lane = iota((ROWS, LANES), 1)
    squares = jnp.where(lane == 0, high, jnp.where(lane == 1, low, 0.0)).astype(bf16)
    gate = matmul(scaled, gate_ref[...]).astype(bf16)
    up = matmul(scaled, up_ref[...]).astype(bf16)
    tiles = gate.shape[1] // LANES
    for k in range(tiles):
        for half in range(2):
            rows = slice(half * 8, half * 8 + 8)
            cols = slice(k * LANES, (k + 1) * LANES)
            out_ref[2 * k + half, 0:8] = gate[rows, cols]
            out_ref[2 * k + half, 8:16] = up[rows, cols]
            out_ref[2 * k + half, 16:24] = squares[rows]
    spare = out_ref.shape[0] - 2 * tiles
    out_ref[2 * tiles :] = jnp.zeros((spare, 24, LANES), bf16)


def first_units(blocks_ref, gain_ref, gate_ref, up_ref, out_ref, stream_ref):
    stream = jnp.sum(blocks_ref[...].astype(f32), axis=0).astype(bf16)
    stream_ref[...] = stream
    send_units(stream, gain_ref, gate_ref, up_ref, out_ref)


def last_units(blocks_ref, before_ref, gain_ref, gate_ref, up_ref, out_ref, stream_ref):
    stream = (before_ref[...].astype(f32) + jnp.sum(blocks_ref[...], axis=0)).astype(bf16)
    stream_ref[...] = stream
    send_units(stream, gain_ref, gate_ref, up_ref, out_ref)


def gate_units(parts_ref, out_ref):
    total = jnp.sum(parts_ref[...].astype(f32), axis=0)
    squares = jnp.sum(total[16:24], axis=1, keepdims=True)
    inv_rms = lax.rsqrt(squares / WIDTH + epsilon)
    hidden = (jax.nn.silu(total[0:8] * inv_rms) * (total[8:16] * inv_rms)).astype(bf16)
    out_ref[...] = jnp.broadcast_to(hidden[None], out_ref.shape)


def sum_down(hidden_ref, down_ref, out_ref):
    tiles = down_ref.shape[0] // LANES
    hidden = jnp.concatenate(
        [
            jnp.concatenate([hidden_ref[2 * k], hidden_ref[2 * k + 1]], axis=0)
            for k in range(tiles)
        ],
        axis=1,
    )
    part = matmul(hidden, down_ref[...])
    out_ref[...] = jnp.broadcast_to(part[None], out_ref.shape)


def send_heads(
    blocks_ref, tokens_ref, gain_ref, query_ref, key_ref, value_ref, out_ref, stream_ref
):
    branch = jnp.sum(blocks_ref[...], axis=0)
    stream = (tokens_ref[...].astype(f32) + 0.5 * branch).astype(bf16)
    stream_ref[...] = stream
    wide = stream.astype(f32)
    high, low = halves(jnp.sum(wide * wide, axis=1, keepdims=True))
    lane = iota((8, LANES), 1)
    squares = jnp.where(lane == 0, high[0:8], jnp.where(lane == 1, low[0:8], 0.0))
    squares = jnp.where(lane == 2, high[8:16], jnp.where(lane == 3, low[8:16], squares))
    scaled = (wide * gain_ref[...]).astype(bf16)
    heads = query_ref.shape[1] // LANES

    def stacked(products):
        return [products[:, h * LANES : (h + 1) * LANES] for h in range(heads)]

    query = stacked(matmul(scaled, query_ref[...]).astype(bf16))
    key = stacked(matmul(scaled, key_ref[...]).astype(bf16))
    value = stacked(matmul(scaled, value_ref[...]).astype(bf16))
    fresh = jnp.concatenate(key + value, axis=0)
    row, col = iota((LANES, LANES), 0), iota((LANES, LANES), 1)
    order = (col == (row % 8) * ROWS + row // 8).astype(bf16)
    fresh = matmul(order, fresh).astype(bf16)
    devices = out_ref.shape[0]
    query = jnp.concatenate(query, axis=0)
    out_ref[:, 0:64] = jnp.broadcast_to(query[None], (devices, 64, LANES))
    out_ref[0:ROWS, 64:72] = fresh.reshape(ROWS, 8, LANES)
    out_ref[ROWS:, 64:72] = jnp.zeros((devices - ROWS, 8, LANES), bf16)
    out_ref[:, 72:80] = jnp.broadcast_to(squares.astype(bf16)[None], (devices, 8, LANES))


def attend(lengths_ref, parts_ref, keys_ref, values_ref, out_ref, own_ref, held_ref):
    total = jnp.sum(parts_ref[...].astype(f32), axis=0)
    squares = total[72:80]
    squares = jnp.concatenate(
        [
            jnp.sum(squares[:, 0:2], axis=1, keepdims=True),
            jnp.sum(squares[:, 2:4], axis=1, keepdims=True),
        ],
        axis=0,
    )
    inv_rms = lax.rsqrt(squares / WIDTH + epsilon)
    query = (total[0:64] * jnp.concatenate([inv_rms] * 4, axis=0)).astype(bf16)
    row, col = iota((LANES, 64), 0), iota((LANES, 64), 1)
    order = (col == (row % 8) // 2 * ROWS + row // 8).astype(bf16)
    query = matmul(order, query)
    row, lane = iota((LANES, LANES), 0), iota((LANES, LANES), 1)
    query = jnp.where(lane // HEAD_DIM == row % 2, query, 0.0)
    held_ref[...] = query
    place = kv_index()
    own = jnp.sum(jnp.where(iota((ROWS, 1), 0) == place, inv_rms, 0.0), axis=0, keepdims=True)
    own_ref[0:8] = (total[64:72] * own).astype(bf16).astype(f32)
    own_ref[8:16] = held_ref[pl.ds(pl.multiple_of(lax.rem(place, ROWS) * 8, 8), 8), :]
    query = query.astype(bf16)
    columns = keys_ref.shape[1]
    positions = columns // 4
    offset = place * positions
    col = iota((8, columns), 1)
    same_head = col % 4 == iota((8, columns), 0) // 2
    position = col // 4 + offset
    stat_lane = iota((8, LANES), 1)
    for b in range(ROWS):
        scores = (
            lax.dot_general(
                query[b * 8 : b * 8 + 8],
                keys_ref[b],
                (((1,), (1,)), ((), ())),
                preferred_element_type=f32,
            )
            * HEAD_DIM**-0.5
        )
        live = same_head & (position < lengths_ref[b])
        scores = jnp.where(live, scores, neg_fill)
        peak = jnp.max(scores, axis=1, keepdims=True)
        weights = jnp.where(live, jnp.exp(scores - peak), 0.0)
        amount = jnp.sum(weights, axis=1, keepdims=True)
        weighted = matmul(weights.astype(bf16), values_ref[b])
        stats = jnp.zeros((8, LANES), f32)
        for k, part in enumerate(thirds(peak) + thirds(amount)):
            stats = jnp.where(stat_lane == k, part, stats)
        out_ref[b, 0:8] = weighted.astype(bf16)
        out_ref[b, 8:16] = stats.astype(bf16)
    out_ref[ROWS:] = jnp.zeros((out_ref.shape[0] - ROWS, 16, LANES), bf16)


def merge(parts_ref, own_ref, lam_ref, gain_ref, out_ref):
    devices = parts_ref.shape[0]
    stats = parts_ref[:, 8:16].reshape(devices * 8, LANES)
    row, col = iota((LANES, 2 * LANES), 0), iota((LANES, 2 * LANES), 1)
    pick = (row // 3 == col // LANES).astype(bf16)
    stats = matmul(stats, pick)
    peaks = stats[:, 0:LANES].reshape(devices, 8, LANES)
    amounts = stats[:, LANES:].reshape(devices, 8, LANES)
    fresh = own_ref[0:8].astype(bf16)
    query = own_ref[8:16]
    row, col = iota((8, 8), 0), iota((8, 8), 1)
    key = matmul((col == row // 2).astype(bf16), fresh)
    value = matmul((col == row // 2 + 4).astype(bf16), fresh)
    self_score = jnp.sum(query * key, axis=1, keepdims=True) * HEAD_DIM**-0.5
    highest = jnp.maximum(jnp.max(peaks, axis=0), self_score)
    scale = jnp.exp(peaks - highest[None])
    own_weight = jnp.exp(self_score - highest)
    amount = jnp.sum(scale * amounts, axis=0) + own_weight
    weighted = jnp.sum(scale * parts_ref[:, 0:8].astype(f32), axis=0)
    weighted = weighted + own_weight.astype(bf16).astype(f32) * value
    ratio = weighted / amount
    row, lane = iota((8, 4), 0), iota((8, 4), 1)
    lam = jnp.sum(jnp.where(lane == row // 2, lam_ref[...], 0.0), axis=1, keepdims=True)
    row = iota((8, LANES), 0)
    ratio = jnp.where(row % 2 == 0, ratio, -lam * ratio)
    mixed = ratio + pltpu.roll(ratio, 7, 0)
    spread = jnp.mean(mixed * mixed, axis=1, keepdims=True)
    normed = mixed * lax.rsqrt(spread + epsilon) * gain_ref[...]
    attended = jnp.where(row % 2 == 0, normed, 0.0).astype(bf16)
    out_ref[...] = jnp.broadcast_to(attended[None], out_ref.shape)


def sum_heads(attended_ref, weight_ref, out_ref):
    rows = attended_ref[0:ROWS].reshape(LANES, LANES)
    row, col = iota((64, LANES), 0), iota((64, LANES), 1)
    order = (col == (row % ROWS) * 8 + row // ROWS * 2).astype(bf16)
    rows = matmul(order, rows).astype(bf16)
    attended = jnp.concatenate([rows[h * ROWS : (h + 1) * ROWS] for h in range(4)], axis=1)
    part = matmul(attended, weight_ref[...])
    out_ref[...] = jnp.broadcast_to(part[None], out_ref.shape)


def finish(blocks_ref, before_ref, out_ref):
    branch = jnp.sum(blocks_ref[...], axis=0)
    stream = (before_ref[...].astype(f32) + 0.5 * branch).astype(bf16)
    own = lax.dot_general(
        stream, own_columns(0), (((1,), (1,)), ((), ())), preferred_element_type=f32
    )
    out_ref[...] = own.astype(bf16)


def on_device(
    tokens,
    first_gain,
    first_gate,
    first_up,
    first_down,
    mixer_gain,
    w_query,
    w_key,
    w_value,
    w_output,
    lam_heads,
    head_gain,
    key_cache,
    value_cache,
    lengths,
    last_gain,
    last_gate,
    last_up,
    last_down,
):
    kv, tp = lax.axis_size(KV), lax.axis_size("tp")
    stream_like = like((ROWS, LANES), bf16)
    units_like = like((kv, 24, LANES), bf16)
    tile_like = like((kv, 8, LANES), bf16)
    sums_like = like((tp, ROWS, LANES), f32)

    def hidden_sums(units, down_w):
        hidden = in_kernel(gate_units, tile_like, swap(units, KV))
        return swap(in_kernel(sum_down, sums_like, swap(hidden, KV), down_w), "tp")

    blocks = swap(in_kernel(spread_tokens, like((tp, ROWS, LANES), bf16), tokens), "tp")
    units, stream = in_kernel(
        first_units,
        (units_like, stream_like),
        blocks,
        first_gain.reshape(1, LANES),
        first_gate,
        first_up,
    )
    heads, first = in_kernel(
        send_heads,
        (like((kv, 80, LANES), bf16), stream_like),
        hidden_sums(units, first_down),
        stream,
        mixer_gain.reshape(1, LANES),
        w_query,
        w_key,
        w_value,
    )
    rows, local, shard_heads, _ = key_cache.shape
    parts, own = pl.pallas_call(
        attend,
        out_shape=(like((kv, 16, LANES), bf16), like((16, LANES), f32)),
        in_specs=[pl.BlockSpec(memory_space=pltpu.SMEM)]
        + [pl.BlockSpec(memory_space=pltpu.VMEM)] * 3,
        out_specs=(pl.BlockSpec(memory_space=pltpu.VMEM),) * 2,
        scratch_shapes=[pltpu.VMEM((LANES, LANES), f32)],
        compiler_params=pltpu.CompilerParams(vmem_limit_bytes=32 << 20),
        name="attend",
    )(
        lengths,
        swap(heads, KV),
        key_cache.reshape(rows, local * shard_heads, LANES),
        value_cache.reshape(rows, local * shard_heads, LANES),
    )
    attended = in_kernel(
        merge,
        tile_like,
        swap(parts, KV),
        own,
        lam_heads.reshape(1, shard_heads),
        head_gain.reshape(1, LANES),
    )
    sums = swap(in_kernel(sum_heads, sums_like, swap(attended, KV), w_output), "tp")
    units, second = in_kernel(
        last_units,
        (units_like, stream_like),
        sums,
        first,
        last_gain.reshape(1, LANES),
        last_gate,
        last_up,
    )
    return in_kernel(
        finish, like((ROWS, ROWS), bf16), hidden_sums(units, last_down), second
    )


def solution(mesh):
    finer = Mesh(mesh.devices.reshape(8, 4, mesh.shape["tp"]), ("kv_0", "kv_1", "tp"))
    return jax.shard_map(
        on_device,
        mesh=finer,
        in_specs=(
            P(None, KV_TP),
            P(KV),
            P(KV, "tp"),
            P(KV, "tp"),
            P("tp", KV),
            P(KV),
            P(KV, "tp"),
            P(KV, "tp"),
            P(KV, "tp"),
            P("tp", KV),
            P("tp"),
            P(),
            P(None, KV, "tp", None),
            P(None, KV, "tp", None),
            P(),
            P(KV),
            P(KV, "tp"),
            P(KV, "tp"),
            P("tp", KV),
        ),
        out_specs=P(None, KV_TP),
        check_vma=False,
    )
```

```python
import functools

import jax
import jax.numpy as jnp
from jax import lax
from jax.experimental import pallas as pl
from jax.experimental.pallas import tpu as pltpu
from jax.sharding import Mesh
from jax.sharding import PartitionSpec as P

WIDTH = 4096
ROWS = 16
HEAD_DIM = 64
LANES = 128
KV = ("kv_0", "kv_1")
KV_TP = ("kv_0", "kv_1", "tp")

epsilon = 1e-06
neg_fill = -1e30
f32 = jnp.float32
bf16 = jnp.bfloat16
covering = pl.CostEstimate(flops=10**10, bytes_accessed=10**5, transcendentals=0)


def iota(shape, dim):
    return lax.broadcasted_iota(jnp.int32, shape, dim)


def matmul(a, b):
    return jnp.dot(a, b, preferred_element_type=f32)


def in_kernel(body, outs, *args, smem=(), vmem_limit=16 << 20):
    spaces = [pltpu.SMEM if k in smem else pltpu.VMEM for k in range(len(args))]
    return pl.pallas_call(
        body,
        out_shape=outs,
        in_specs=[pl.BlockSpec(memory_space=space) for space in spaces],
        out_specs=jax.tree.map(lambda _: pl.BlockSpec(memory_space=pltpu.VMEM), outs),
        compiler_params=pltpu.CompilerParams(vmem_limit_bytes=vmem_limit),
        cost_estimate=covering,
        name=body.__name__,
    )(*args)


def swap(blocks, axis):
    return lax.all_to_all(blocks, axis, split_axis=0, concat_axis=0, tiled=True)


def like(shape, kind):
    return jax.ShapeDtypeStruct(shape, kind)


def kv_index():
    return lax.axis_index("kv_0") * lax.axis_size("kv_1") + lax.axis_index("kv_1")


def halves(column):
    high = column.astype(bf16)
    low = (column - high.astype(f32)).astype(bf16)
    return high.astype(f32), low.astype(f32)


def thirds(column):
    high, low = halves(column)
    rest = (column - high) - low
    return high, low, rest


def own_columns(shape_dim):
    place = lax.axis_index("tp") * ROWS
    return (iota((ROWS, LANES), 1) == iota((ROWS, LANES), 0) + place).astype(bf16)


def spread_tokens(tokens_ref, out_ref):
    block = matmul(tokens_ref[...], own_columns(0)).astype(bf16)
    out_ref[...] = jnp.broadcast_to(block[None], out_ref.shape)


def send_units(stream, gain_ref, gate_ref, up_ref, out_ref):
    wide = stream.astype(f32)
    high, low = halves(jnp.sum(wide * wide, axis=1, keepdims=True))
    scaled = (wide * gain_ref[...]).astype(bf16)
    lane = iota((ROWS, LANES), 1)
    squares = jnp.where(lane == 0, high, jnp.where(lane == 1, low, 0.0)).astype(bf16)
    gate = matmul(scaled, gate_ref[...]).astype(bf16)
    up = matmul(scaled, up_ref[...]).astype(bf16)
    tiles = gate.shape[1] // LANES
    for k in range(tiles):
        for half in range(2):
            rows = slice(half * 8, half * 8 + 8)
            cols = slice(k * LANES, (k + 1) * LANES)
            out_ref[2 * k + half, 0:8] = gate[rows, cols]
            out_ref[2 * k + half, 8:16] = up[rows, cols]
            out_ref[2 * k + half, 16:24] = squares[rows]
    spare = out_ref.shape[0] - 2 * tiles
    out_ref[2 * tiles :] = jnp.zeros((spare, 24, LANES), bf16)


def first_units(blocks_ref, gain_ref, gate_ref, up_ref, out_ref, stream_ref):
    stream = jnp.sum(blocks_ref[...].astype(f32), axis=0).astype(bf16)
    stream_ref[...] = stream
    send_units(stream, gain_ref, gate_ref, up_ref, out_ref)


def last_units(blocks_ref, before_ref, gain_ref, gate_ref, up_ref, out_ref, stream_ref):
    stream = (before_ref[...].astype(f32) + jnp.sum(blocks_ref[...], axis=0)).astype(bf16)
    stream_ref[...] = stream
    send_units(stream, gain_ref, gate_ref, up_ref, out_ref)


def gate_units(parts_ref, out_ref):
    total = jnp.sum(parts_ref[...].astype(f32), axis=0)
    squares = jnp.sum(total[16:24], axis=1, keepdims=True)
    inv_rms = lax.rsqrt(squares / WIDTH + epsilon)
    hidden = (jax.nn.silu(total[0:8] * inv_rms) * (total[8:16] * inv_rms)).astype(bf16)
    out_ref[...] = jnp.broadcast_to(hidden[None], out_ref.shape)


def sum_down(hidden_ref, down_ref, out_ref):
    tiles = down_ref.shape[0] // LANES
    hidden = jnp.concatenate(
        [
            jnp.concatenate([hidden_ref[2 * k], hidden_ref[2 * k + 1]], axis=0)
            for k in range(tiles)
        ],
        axis=1,
    )
    part = matmul(hidden, down_ref[...])
    out_ref[...] = jnp.broadcast_to(part[None], out_ref.shape)


def send_heads(
    blocks_ref, tokens_ref, gain_ref, query_ref, key_ref, value_ref, out_ref, stream_ref
):
    branch = jnp.sum(blocks_ref[...], axis=0)
    stream = (tokens_ref[...].astype(f32) + 0.5 * branch).astype(bf16)
    stream_ref[...] = stream
    wide = stream.astype(f32)
    high, low = halves(jnp.sum(wide * wide, axis=1, keepdims=True))
    lane = iota((8, LANES), 1)
    squares = jnp.where(lane == 0, high[0:8], jnp.where(lane == 1, low[0:8], 0.0))
    squares = jnp.where(lane == 2, high[8:16], jnp.where(lane == 3, low[8:16], squares))
    scaled = (wide * gain_ref[...]).astype(bf16)
    heads = query_ref.shape[1] // LANES

    def stacked(products):
        return [products[:, h * LANES : (h + 1) * LANES] for h in range(heads)]

    query = stacked(matmul(scaled, query_ref[...]).astype(bf16))
    key = stacked(matmul(scaled, key_ref[...]).astype(bf16))
    value = stacked(matmul(scaled, value_ref[...]).astype(bf16))
    fresh = jnp.concatenate(key + value, axis=0)
    row, col = iota((LANES, LANES), 0), iota((LANES, LANES), 1)
    order = (col == (row % 8) * ROWS + row // 8).astype(bf16)
    fresh = matmul(order, fresh).astype(bf16)
    devices = out_ref.shape[0]
    query = jnp.concatenate(query, axis=0)
    out_ref[:, 0:64] = jnp.broadcast_to(query[None], (devices, 64, LANES))
    out_ref[0:ROWS, 64:72] = fresh.reshape(ROWS, 8, LANES)
    out_ref[ROWS:, 64:72] = jnp.zeros((devices - ROWS, 8, LANES), bf16)
    out_ref[:, 72:80] = jnp.broadcast_to(squares.astype(bf16)[None], (devices, 8, LANES))


def attend(lengths_ref, parts_ref, keys_ref, values_ref, out_ref, own_ref, held_ref):
    total = jnp.sum(parts_ref[...].astype(f32), axis=0)
    squares = total[72:80]
    squares = jnp.concatenate(
        [
            jnp.sum(squares[:, 0:2], axis=1, keepdims=True),
            jnp.sum(squares[:, 2:4], axis=1, keepdims=True),
        ],
        axis=0,
    )
    inv_rms = lax.rsqrt(squares / WIDTH + epsilon)
    query = (total[0:64] * jnp.concatenate([inv_rms] * 4, axis=0)).astype(bf16)
    row, col = iota((LANES, 64), 0), iota((LANES, 64), 1)
    order = (col == (row % 8) // 2 * ROWS + row // 8).astype(bf16)
    query = matmul(order, query)
    row, lane = iota((LANES, LANES), 0), iota((LANES, LANES), 1)
    query = jnp.where(lane // HEAD_DIM == row % 2, query, 0.0)
    held_ref[...] = query
    place = kv_index()
    own = jnp.sum(jnp.where(iota((ROWS, 1), 0) == place, inv_rms, 0.0), axis=0, keepdims=True)
    own_ref[0:8] = (total[64:72] * own).astype(bf16).astype(f32)
    own_ref[8:16] = held_ref[pl.ds(pl.multiple_of(lax.rem(place, ROWS) * 8, 8), 8), :]
    query = query.astype(bf16)
    columns = keys_ref.shape[1]
    positions = columns // 4
    offset = place * positions
    col = iota((8, columns), 1)
    same_head = col % 4 == iota((8, columns), 0) // 2
    position = col // 4 + offset
    stat_lane = iota((8, LANES), 1)
    for b in range(ROWS):
        scores = (
            lax.dot_general(
                query[b * 8 : b * 8 + 8],
                keys_ref[b],
                (((1,), (1,)), ((), ())),
                preferred_element_type=f32,
            )
            * HEAD_DIM**-0.5
        )
        live = same_head & (position < lengths_ref[b])
        scores = jnp.where(live, scores, neg_fill)
        peak = jnp.max(scores, axis=1, keepdims=True)
        weights = jnp.where(live, jnp.exp(scores - peak), 0.0)
        amount = jnp.sum(weights, axis=1, keepdims=True)
        weighted = matmul(weights.astype(bf16), values_ref[b])
        stats = jnp.zeros((8, LANES), f32)
        for k, part in enumerate(thirds(peak) + thirds(amount)):
            stats = jnp.where(stat_lane == k, part, stats)
        out_ref[b, 0:8] = weighted.astype(bf16)
        out_ref[b, 8:16] = stats.astype(bf16)
    out_ref[ROWS:] = jnp.zeros((out_ref.shape[0] - ROWS, 16, LANES), bf16)


def merge(parts_ref, own_ref, lam_ref, gain_ref, out_ref):
    devices = parts_ref.shape[0]
    stats = parts_ref[:, 8:16].reshape(devices * 8, LANES)
    row, col = iota((LANES, 2 * LANES), 0), iota((LANES, 2 * LANES), 1)
    pick = (row // 3 == col // LANES).astype(bf16)
    stats = matmul(stats, pick)
    peaks = stats[:, 0:LANES].reshape(devices, 8, LANES)
    amounts = stats[:, LANES:].reshape(devices, 8, LANES)
    fresh = own_ref[0:8].astype(bf16)
    query = own_ref[8:16]
    row, col = iota((8, 8), 0), iota((8, 8), 1)
    key = matmul((col == row // 2).astype(bf16), fresh)
    value = matmul((col == row // 2 + 4).astype(bf16), fresh)
    self_score = jnp.sum(query * key, axis=1, keepdims=True) * HEAD_DIM**-0.5
    highest = jnp.maximum(jnp.max(peaks, axis=0), self_score)
    scale = jnp.exp(peaks - highest[None])
    own_weight = jnp.exp(self_score - highest)
    amount = jnp.sum(scale * amounts, axis=0) + own_weight
    weighted = jnp.sum(scale * parts_ref[:, 0:8].astype(f32), axis=0)
    weighted = weighted + own_weight.astype(bf16).astype(f32) * value
    ratio = weighted / amount
    row, lane = iota((8, 4), 0), iota((8, 4), 1)
    lam = jnp.sum(jnp.where(lane == row // 2, lam_ref[...], 0.0), axis=1, keepdims=True)
    row = iota((8, LANES), 0)
    ratio = jnp.where(row % 2 == 0, ratio, -lam * ratio)
    mixed = ratio + pltpu.roll(ratio, 7, 0)
    spread = jnp.mean(mixed * mixed, axis=1, keepdims=True)
    normed = mixed * lax.rsqrt(spread + epsilon) * gain_ref[...]
    attended = jnp.where(row % 2 == 0, normed, 0.0).astype(bf16)
    out_ref[...] = jnp.broadcast_to(attended[None], out_ref.shape)


def sum_heads(attended_ref, weight_ref, out_ref):
    rows = attended_ref[0:ROWS].reshape(LANES, LANES)
    row, col = iota((64, LANES), 0), iota((64, LANES), 1)
    order = (col == (row % ROWS) * 8 + row // ROWS * 2).astype(bf16)
    rows = matmul(order, rows).astype(bf16)
    attended = jnp.concatenate([rows[h * ROWS : (h + 1) * ROWS] for h in range(4)], axis=1)
    part = matmul(attended, weight_ref[...])
    out_ref[...] = jnp.broadcast_to(part[None], out_ref.shape)


def finish(blocks_ref, before_ref, out_ref):
    branch = jnp.sum(blocks_ref[...], axis=0)
    stream = (before_ref[...].astype(f32) + 0.5 * branch).astype(bf16)
    own = lax.dot_general(
        stream, own_columns(0), (((1,), (1,)), ((), ())), preferred_element_type=f32
    )
    out_ref[...] = own.astype(bf16)


def on_device(
    tokens,
    first_gain,
    first_gate,
    first_up,
    first_down,
    mixer_gain,
    w_query,
    w_key,
    w_value,
    w_output,
    lam_heads,
    head_gain,
    key_cache,
    value_cache,
    lengths,
    last_gain,
    last_gate,
    last_up,
    last_down,
):
    kv, tp = lax.axis_size(KV), lax.axis_size("tp")
    stream_like = like((ROWS, LANES), bf16)
    units_like = like((kv, 24, LANES), bf16)
    tile_like = like((kv, 8, LANES), bf16)
    sums_like = like((tp, ROWS, LANES), f32)

    def hidden_sums(units, down_w):
        hidden = in_kernel(gate_units, tile_like, swap(units, KV))
        return swap(in_kernel(sum_down, sums_like, swap(hidden, KV), down_w), "tp")

    blocks = swap(in_kernel(spread_tokens, like((tp, ROWS, LANES), bf16), tokens), "tp")
    units, stream = in_kernel(
        first_units,
        (units_like, stream_like),
        blocks,
        first_gain.reshape(1, LANES),
        first_gate,
        first_up,
    )
    heads, first = in_kernel(
        send_heads,
        (like((kv, 80, LANES), bf16), stream_like),
        hidden_sums(units, first_down),
        stream,
        mixer_gain.reshape(1, LANES),
        w_query,
        w_key,
        w_value,
    )
    rows, local, shard_heads, _ = key_cache.shape
    parts, own = pl.pallas_call(
        attend,
        out_shape=(like((kv, 16, LANES), bf16), like((16, LANES), f32)),
        in_specs=[pl.BlockSpec(memory_space=pltpu.SMEM)]
        + [pl.BlockSpec(memory_space=pltpu.VMEM)] * 3,
        out_specs=(pl.BlockSpec(memory_space=pltpu.VMEM),) * 2,
        scratch_shapes=[pltpu.VMEM((LANES, LANES), f32)],
        compiler_params=pltpu.CompilerParams(vmem_limit_bytes=32 << 20),
        cost_estimate=covering,
        name="attend",
    )(
        lengths,
        swap(heads, KV),
        key_cache.reshape(rows, local * shard_heads, LANES),
        value_cache.reshape(rows, local * shard_heads, LANES),
    )
    attended = in_kernel(
        merge,
        tile_like,
        swap(parts, KV),
        own,
        lam_heads.reshape(1, shard_heads),
        head_gain.reshape(1, LANES),
    )
    sums = swap(in_kernel(sum_heads, sums_like, swap(attended, KV), w_output), "tp")
    units, second = in_kernel(
        last_units,
        (units_like, stream_like),
        sums,
        first,
        last_gain.reshape(1, LANES),
        last_gate,
        last_up,
    )
    return in_kernel(
        finish, like((ROWS, ROWS), bf16), hidden_sums(units, last_down), second
    )


def solution(mesh):
    finer = Mesh(mesh.devices.reshape(8, 4, mesh.shape["tp"]), ("kv_0", "kv_1", "tp"))
    return jax.shard_map(
        on_device,
        mesh=finer,
        in_specs=(
            P(None, KV_TP),
            P(KV),
            P(KV, "tp"),
            P(KV, "tp"),
            P("tp", KV),
            P(KV),
            P(KV, "tp"),
            P(KV, "tp"),
            P(KV, "tp"),
            P("tp", KV),
            P("tp"),
            P(),
            P(None, KV, "tp", None),
            P(None, KV, "tp", None),
            P(),
            P(KV),
            P(KV, "tp"),
            P(KV, "tp"),
            P("tp", KV),
        ),
        out_specs=P(None, KV_TP),
        check_vma=False,
    )
```

```python
import functools

import jax
import jax.numpy as jnp
from jax import lax
from jax.experimental import pallas as pl
from jax.experimental.pallas import tpu as pltpu
from jax.sharding import Mesh
from jax.sharding import PartitionSpec as P

WIDTH = 4096
ROWS = 16
HEAD_DIM = 64
LANES = 128
KV = ("kv_0", "kv_1")
KV_TP = ("kv_0", "kv_1", "tp")


epsilon = 1e-06
neg_fill = -1e30
f32 = jnp.float32
bf16 = jnp.bfloat16
covering = pl.CostEstimate(flops=10**10, bytes_accessed=10**5, transcendentals=0)


def iota(shape, dim):
    return lax.broadcasted_iota(jnp.int32, shape, dim)


def matmul(a, b):
    return jnp.dot(a, b, preferred_element_type=f32)


def in_kernel(body, outs, *args, smem=(), scratch=(), vmem_limit=16 << 20):
    spaces = [pltpu.SMEM if k in smem else pltpu.VMEM for k in range(len(args))]
    return pl.pallas_call(
        body,
        out_shape=outs,
        in_specs=[pl.BlockSpec(memory_space=space) for space in spaces],
        out_specs=jax.tree.map(lambda _: pl.BlockSpec(memory_space=pltpu.VMEM), outs),
        scratch_shapes=scratch,
        compiler_params=pltpu.CompilerParams(vmem_limit_bytes=vmem_limit),
        cost_estimate=covering,
        name=body.__name__,
    )(*args)


def swap(blocks, axis):
    return lax.all_to_all(blocks, axis, split_axis=0, concat_axis=0, tiled=True)


def like(shape, kind):
    return jax.ShapeDtypeStruct(shape, kind)


def kv_index():
    return lax.axis_index("kv_0") * lax.axis_size("kv_1") + lax.axis_index("kv_1")


def halves(column):
    high = column.astype(bf16)
    low = (column - high.astype(f32)).astype(bf16)
    return high.astype(f32), low.astype(f32)


def thirds(column):
    high, low = halves(column)
    rest = (column - high) - low
    return high, low, rest


def own_columns(shape_dim):
    place = lax.axis_index("tp") * ROWS
    return (iota((ROWS, LANES), 1) == iota((ROWS, LANES), 0) + place).astype(bf16)


def spread_tokens(tokens_ref, out_ref):
    block = matmul(tokens_ref[...], own_columns(0)).astype(bf16)
    out_ref[...] = jnp.broadcast_to(block[None], out_ref.shape)


def send_units(stream, gain_ref, gate_ref, up_ref, out_ref):
    wide = stream.astype(f32)
    high, low = halves(jnp.sum(wide * wide, axis=1, keepdims=True))
    scaled = (wide * gain_ref[...]).astype(bf16)
    lane = iota((ROWS, LANES), 1)
    squares = jnp.where(lane == 0, high, jnp.where(lane == 1, low, 0.0)).astype(bf16)
    gate = matmul(scaled, gate_ref[...]).astype(bf16)
    up = matmul(scaled, up_ref[...]).astype(bf16)
    tiles = gate.shape[1] // LANES
    for k in range(tiles):
        for half in range(2):
            rows = slice(half * 8, half * 8 + 8)
            cols = slice(k * LANES, (k + 1) * LANES)
            out_ref[2 * k + half, 0:8] = gate[rows, cols]
            out_ref[2 * k + half, 8:16] = up[rows, cols]
            out_ref[2 * k + half, 16:24] = squares[rows]
    spare = out_ref.shape[0] - 2 * tiles
    out_ref[2 * tiles :] = jnp.zeros((spare, 24, LANES), bf16)


def first_units(blocks_ref, gain_ref, gate_ref, up_ref, out_ref, stream_ref):
    stream = jnp.sum(blocks_ref[...].astype(f32), axis=0).astype(bf16)
    stream_ref[...] = stream
    send_units(stream, gain_ref, gate_ref, up_ref, out_ref)


def last_units(blocks_ref, before_ref, gain_ref, gate_ref, up_ref, out_ref, stream_ref):
    stream = (before_ref[...].astype(f32) + jnp.sum(blocks_ref[...], axis=0)).astype(bf16)
    stream_ref[...] = stream
    send_units(stream, gain_ref, gate_ref, up_ref, out_ref)


def gate_units(parts_ref, out_ref):
    total = jnp.sum(parts_ref[...].astype(f32), axis=0)
    squares = jnp.sum(total[16:24], axis=1, keepdims=True)
    inv_rms = lax.rsqrt(squares / WIDTH + epsilon)
    hidden = (jax.nn.silu(total[0:8] * inv_rms) * (total[8:16] * inv_rms)).astype(bf16)
    out_ref[...] = jnp.broadcast_to(hidden[None], out_ref.shape)


def sum_down(hidden_ref, down_ref, out_ref):
    tiles = down_ref.shape[0] // LANES
    hidden = jnp.concatenate(
        [
            jnp.concatenate([hidden_ref[2 * k], hidden_ref[2 * k + 1]], axis=0)
            for k in range(tiles)
        ],
        axis=1,
    )
    part = matmul(hidden, down_ref[...])
    out_ref[...] = jnp.broadcast_to(part[None], out_ref.shape)


def rotations(array, axis):
    devices = lax.axis_size(axis)
    return [array] + [
        lax.ppermute(array, axis, [(k, (k + turn) % devices) for k in range(devices)])
        for turn in range(1, devices)
    ]


def in_pairs(values):
    own, one, two, three = values
    return (own + two) + (one + three)


def as_row(column):
    size = column.shape[0]
    same = iota((size, LANES), 0) == iota((size, LANES), 1)
    return jnp.sum(jnp.where(same, column, 0.0), axis=0, keepdims=True)


def as_rows(parts):
    row = iota((8, LANES), 0)
    stacked = jnp.zeros((8, LANES), f32)
    for k, part in enumerate(parts):
        stacked = jnp.where(row == k, part, stacked)
    return stacked


def send_heads(
    blocks_ref, tokens_ref, gain_ref, query_ref, key_ref, value_ref, out_ref, stream_ref
):
    branch = jnp.sum(blocks_ref[...], axis=0)
    stream = (tokens_ref[...].astype(f32) + 0.5 * branch).astype(bf16)
    stream_ref[...] = stream
    wide = stream.astype(f32)
    squares = as_row(jnp.sum(wide * wide, axis=1, keepdims=True))
    scaled = (wide * gain_ref[...]).astype(bf16)
    at = 0
    for weight_ref in (query_ref, key_ref, value_ref):
        product = matmul(scaled, weight_ref[...]).astype(bf16)
        for h in range(product.shape[1] // LANES):
            out_ref[at : at + ROWS] = product[:, h * LANES : (h + 1) * LANES]
            at += ROWS
    out_ref[at:] = as_rows(halves(squares)).astype(bf16)


def share_heads(own_ref, one_ref, two_ref, three_ref, out_ref):
    total = in_pairs([ref[...].astype(f32) for ref in (own_ref, one_ref, two_ref, three_ref)])
    query = total[0:64].astype(bf16)
    fresh = total[64:192].astype(bf16)
    squares = total[192:193] + total[193:194]
    groups = out_ref.shape[0]
    row, col = iota((groups * 8, LANES), 0), iota((groups * 8, LANES), 1)
    part = row % 8
    place = row // 8 * lax.axis_size("kv_1") + lax.axis_index("kv_1")
    source = ((part // 2) * 4 + (place % 2) * 2 + part % 2) * ROWS + place // 2
    order = ((part < 4) & (col == source)).astype(bf16)
    fresh = matmul(order, fresh).reshape(groups, 8, LANES)
    high, low = halves(squares)
    fresh = fresh + as_rows([0.0] * 4 + [high, low])[None]
    out_ref[:, 0:64] = jnp.broadcast_to(query[None], (groups, 64, LANES))
    out_ref[:, 64:72] = fresh.astype(bf16)


def attend(
    lengths_ref, parts_ref, keys_ref, values_ref, out_ref, scores_ref, weights_ref, stats_ref
):
    total = jnp.sum(parts_ref[...].astype(f32), axis=0)
    squares = total[68:69] + total[69:70]
    token, lane = iota((ROWS, LANES), 0), iota((ROWS, LANES), 1)
    squares = jnp.sum(jnp.where(token == lane, squares, 0.0), axis=1, keepdims=True)
    inv_rms = lax.rsqrt(squares / WIDTH + epsilon)
    query = (total[0:64] * jnp.concatenate([inv_rms] * 4, axis=0)).astype(bf16)
    row, col = iota((LANES, 64), 0), iota((LANES, 64), 1)
    order = (col == (row % 8) // 2 * ROWS + row // 8).astype(bf16)
    query = matmul(order, query)
    row, lane = iota((LANES, LANES), 0), iota((LANES, LANES), 1)
    query = jnp.where(lane // HEAD_DIM == row % 2, query, 0.0)
    place = kv_index()
    own_inv = jnp.sum(
        jnp.where(iota((ROWS, 1), 0) == place // 2, inv_rms, 0.0), axis=0, keepdims=True
    )
    fresh = (total[64:72] * own_inv).astype(bf16)
    row, col = iota((LANES, 8), 0), iota((LANES, 8), 1)
    own_key = matmul((col == row % 4 // 2).astype(bf16), fresh)
    own_value = matmul((col == row % 4 // 2 + 2).astype(bf16), fresh)
    owned = iota((LANES, 1), 0) // 4 == place
    self_score = jnp.sum(query * own_key, axis=1, keepdims=True) * HEAD_DIM**-0.5
    self_score = jnp.where(owned, self_score, neg_fill)
    query = query.astype(bf16)
    columns = keys_ref.shape[1]
    offset = place * (columns // 4)
    col = iota((8, columns), 1)
    same_head = col % 4 == iota((8, columns), 0) // 2
    position = jnp.where(same_head, col // 4 + offset, 1 << 30)
    for b in range(ROWS):
        rows = slice(b * 8, b * 8 + 8)
        scores_ref[rows] = lax.dot_general(
            query[rows],
            keys_ref[b],
            (((1,), (1,)), ((), ())),
            preferred_element_type=f32,
        )
    for b in range(ROWS):
        rows = slice(b * 8, b * 8 + 8)
        live = position < lengths_ref[b]
        scores = jnp.where(live, scores_ref[rows] * HEAD_DIM**-0.5, neg_fill)
        peak = jnp.maximum(jnp.max(scores, axis=1, keepdims=True), self_score[rows])
        weights = jnp.where(live, jnp.exp(scores - peak), 0.0)
        own_weight = jnp.where(owned[rows], jnp.exp(self_score[rows] - peak), 0.0)
        amount = jnp.sum(weights, axis=1, keepdims=True) + own_weight
        weights_ref[rows] = weights.astype(bf16)
        stats_ref[0, rows] = jnp.broadcast_to(peak, (8, LANES))
        stats_ref[1, rows] = jnp.broadcast_to(amount, (8, LANES))
        stats_ref[2, rows] = own_weight.astype(bf16).astype(f32) * own_value[rows]
    for b in range(ROWS):
        rows = slice(b * 8, b * 8 + 8)
        weighted = matmul(weights_ref[rows], values_ref[b]) + stats_ref[2, rows]
        out_ref[rows] = weighted.astype(bf16)
    parts = thirds(as_row(stats_ref[0])) + thirds(as_row(stats_ref[1]))
    out_ref[LANES:] = as_rows(parts).astype(bf16)


def peak_and_amount(stats):
    stats = stats.astype(f32)
    return stats[0:1] + stats[1:2] + stats[2:3], stats[3:4] + stats[4:5] + stats[5:6]


def join(own_ref, one_ref, two_ref, three_ref, out_ref):
    refs = (own_ref, one_ref, two_ref, three_ref)
    peaks, amounts = zip(*[peak_and_amount(ref[LANES:]) for ref in refs])
    highest = functools.reduce(jnp.maximum, peaks)
    scales = [jnp.exp(peak - highest) for peak in peaks]
    amount = in_pairs([scale * amount for scale, amount in zip(scales, amounts)])
    scales = as_rows(scales).T
    weighted = in_pairs(
        [scales[:, k : k + 1] * ref[0:LANES].astype(f32) for k, ref in enumerate(refs)]
    )
    groups = out_ref.shape[0]
    stats = as_rows(thirds(highest) + thirds(amount)).astype(bf16)
    out_ref[:, 0:LANES] = jnp.broadcast_to(weighted.astype(bf16)[None], (groups, LANES, LANES))
    out_ref[:, LANES:] = jnp.broadcast_to(stats[None], (groups, 8, LANES))


def finish_heads(parts_ref, lam_ref, gain_ref, weight_ref, out_ref):
    groups = parts_ref.shape[0]
    peaks, amounts = zip(*[peak_and_amount(parts_ref[k, LANES:]) for k in range(groups)])
    highest = functools.reduce(jnp.maximum, peaks)
    scales = [jnp.exp(peak - highest) for peak in peaks]
    amount = sum(scale * amount for scale, amount in zip(scales, amounts))
    lane = iota((1, LANES), 1)
    share = jnp.ones((1, LANES), f32)
    for h in range(lam_ref.shape[1]):
        share = jnp.where(lane % 8 == 2 * h + 1, -lam_ref[:, h : h + 1], share)
    share = share / amount
    shares = as_rows([scale * share for scale in scales]).T
    ratio = sum(shares[:, k : k + 1] * parts_ref[k, 0:LANES].astype(f32) for k in range(groups))
    mixed = ratio + pltpu.roll(ratio, LANES - 1, 0)
    spread = jnp.mean(mixed * mixed, axis=1, keepdims=True)
    attended = (mixed * lax.rsqrt(spread + epsilon) * gain_ref[...]).astype(bf16)
    row, col = iota((64, LANES), 0), iota((64, LANES), 1)
    order = (col == (row % ROWS) * 8 + row // ROWS * 2).astype(bf16)
    attended = matmul(order, attended).astype(bf16)
    attended = jnp.concatenate(
        [attended[h * ROWS : (h + 1) * ROWS] for h in range(64 // ROWS)], axis=1
    )
    part = matmul(attended, weight_ref[...])
    out_ref[...] = jnp.broadcast_to(part[None], out_ref.shape)


def finish(blocks_ref, before_ref, out_ref):
    branch = jnp.sum(blocks_ref[...], axis=0)
    stream = (before_ref[...].astype(f32) + 0.5 * branch).astype(bf16)
    own = lax.dot_general(
        stream, own_columns(0), (((1,), (1,)), ((), ())), preferred_element_type=f32
    )
    out_ref[...] = own.astype(bf16)


def on_device(
    tokens,
    first_gain,
    first_gate,
    first_up,
    first_down,
    mixer_gain,
    w_query,
    w_key,
    w_value,
    w_output,
    lam_heads,
    head_gain,
    key_cache,
    value_cache,
    lengths,
    last_gain,
    last_gate,
    last_up,
    last_down,
):
    kv, tp = lax.axis_size(KV), lax.axis_size("tp")
    stream_like = like((ROWS, LANES), bf16)
    units_like = like((kv, 24, LANES), bf16)
    tile_like = like((kv, 8, LANES), bf16)
    sums_like = like((tp, ROWS, LANES), f32)

    def hidden_sums(units, down_w):
        hidden = in_kernel(gate_units, tile_like, swap(units, KV))
        return swap(in_kernel(sum_down, sums_like, swap(hidden, KV), down_w), "tp")

    blocks = swap(in_kernel(spread_tokens, like((tp, ROWS, LANES), bf16), tokens), "tp")
    units, stream = in_kernel(
        first_units,
        (units_like, stream_like),
        blocks,
        first_gain.reshape(1, LANES),
        first_gate,
        first_up,
    )
    heads, first = in_kernel(
        send_heads,
        (like((200, LANES), bf16), stream_like),
        hidden_sums(units, first_down),
        stream,
        mixer_gain.reshape(1, LANES),
        w_query,
        w_key,
        w_value,
    )
    planes = lax.axis_size("kv_0")
    heads = in_kernel(share_heads, like((planes, 72, LANES), bf16), *rotations(heads, "kv_1"))
    rows, local, shard_heads, _ = key_cache.shape
    columns = local * shard_heads
    part = in_kernel(
        attend,
        like((LANES + 8, LANES), bf16),
        lengths,
        swap(heads, "kv_0"),
        key_cache.reshape(rows, columns, LANES),
        value_cache.reshape(rows, columns, LANES),
        smem=(0,),
        scratch=(
            pltpu.VMEM((LANES, columns), f32),
            pltpu.VMEM((LANES, columns), bf16),
            pltpu.VMEM((3, LANES, LANES), f32),
        ),
        vmem_limit=32 << 20,
    )
    parts = in_kernel(
        join, like((planes, LANES + 8, LANES), bf16), *rotations(part, "kv_1")
    )
    sums = in_kernel(
        finish_heads,
        sums_like,
        swap(parts, "kv_0"),
        lam_heads.reshape(1, shard_heads),
        head_gain.reshape(1, LANES),
        w_output,
    )
    sums = swap(sums, "tp")
    units, second = in_kernel(
        last_units,
        (units_like, stream_like),
        sums,
        first,
        last_gain.reshape(1, LANES),
        last_gate,
        last_up,
    )
    return in_kernel(
        finish, like((ROWS, ROWS), bf16), hidden_sums(units, last_down), second
    )


def solution(mesh):
    finer = Mesh(mesh.devices.reshape(8, 4, mesh.shape["tp"]), ("kv_0", "kv_1", "tp"))
    return jax.shard_map(
        on_device,
        mesh=finer,
        in_specs=(
            P(None, KV_TP),
            P(KV),
            P(KV, "tp"),
            P(KV, "tp"),
            P("tp", KV),
            P(KV),
            P(KV, "tp"),
            P(KV, "tp"),
            P(KV, "tp"),
            P("tp", KV),
            P("tp"),
            P(),
            P(None, KV, "tp", None),
            P(None, KV, "tp", None),
            P(),
            P(KV),
            P(KV, "tp"),
            P(KV, "tp"),
            P("tp", KV),
        ),
        out_specs=P(None, KV_TP),
        check_vma=False,
    )
```

```python
import functools

import jax
import jax.numpy as jnp
from jax import lax
from jax.experimental import pallas as pl
from jax.experimental.pallas import tpu as pltpu
from jax.sharding import Mesh
from jax.sharding import PartitionSpec as P

WIDTH = 4096
ROWS = 16
HEAD_DIM = 64
LANES = 128
KV = ("kv_0", "kv_1")
KV_TP = ("kv_0", "kv_1", "tp")


epsilon = 1e-06
neg_fill = -1e30
f32 = jnp.float32
bf16 = jnp.bfloat16
covering = pl.CostEstimate(flops=10**10, bytes_accessed=10**5, transcendentals=0)


def iota(shape, dim):
    return lax.broadcasted_iota(jnp.int32, shape, dim)


def matmul(a, b):
    return jnp.dot(a, b, preferred_element_type=f32)


def in_kernel(body, outs, *args, smem=(), scratch=(), vmem_limit=16 << 20):
    spaces = [pltpu.SMEM if k in smem else pltpu.VMEM for k in range(len(args))]
    return pl.pallas_call(
        body,
        out_shape=outs,
        in_specs=[pl.BlockSpec(memory_space=space) for space in spaces],
        out_specs=jax.tree.map(lambda _: pl.BlockSpec(memory_space=pltpu.VMEM), outs),
        scratch_shapes=scratch,
        compiler_params=pltpu.CompilerParams(vmem_limit_bytes=vmem_limit),
        cost_estimate=covering,
        name=body.__name__,
    )(*args)


def swap(blocks, axis):
    return lax.all_to_all(blocks, axis, split_axis=0, concat_axis=0, tiled=True)


def like(shape, kind):
    return jax.ShapeDtypeStruct(shape, kind)


def kv_index():
    return lax.axis_index("kv_0") * lax.axis_size("kv_1") + lax.axis_index("kv_1")


def halves(column):
    high = column.astype(bf16)
    low = (column - high.astype(f32)).astype(bf16)
    return high.astype(f32), low.astype(f32)


def thirds(column):
    high, low = halves(column)
    rest = (column - high) - low
    return high, low, rest


def own_columns(shape_dim):
    place = lax.axis_index("tp") * ROWS
    return (iota((ROWS, LANES), 1) == iota((ROWS, LANES), 0) + place).astype(bf16)


def spread_tokens(tokens_ref, out_ref):
    block = matmul(tokens_ref[...], own_columns(0)).astype(bf16)
    out_ref[...] = jnp.broadcast_to(block[None], out_ref.shape)


def send_units(stream, gain_ref, gate_ref, up_ref, out_refs):
    groups = len(out_refs)
    size = ROWS // groups
    row, col = iota((groups * 8, ROWS), 0), iota((groups * 8, ROWS), 1)
    target = lax.rem(lax.axis_index("kv_1") + row // 8, groups)
    order = (col == target * size + row % size).astype(bf16)
    wide = matmul(order, stream)
    high, low = halves(jnp.sum(wide * wide, axis=1, keepdims=True))
    lane = iota((groups * 8, LANES), 1)
    squares = jnp.where(lane == 0, high, jnp.where(lane == 1, low, 0.0)).astype(bf16)
    scaled = (wide * gain_ref[...]).astype(bf16)
    gate = matmul(scaled, gate_ref[...])
    up = matmul(scaled, up_ref[...])
    both = jnp.where(iota(gate.shape, 0) % 8 < size, gate, up).astype(bf16)
    tiles = both.shape[1] // LANES
    for turn, out_ref in enumerate(out_refs):
        rows = slice(turn * 8, turn * 8 + 8)
        for k in range(tiles):
            out_ref[k * 8 : k * 8 + 8] = both[rows, k * LANES : (k + 1) * LANES]
        out_ref[tiles * 8 :] = squares[rows]


def first_units(blocks_ref, gain_ref, gate_ref, up_ref, stream_ref, *out_refs):
    stream = jnp.sum(blocks_ref[...].astype(f32), axis=0).astype(bf16)
    stream_ref[...] = stream
    send_units(stream, gain_ref, gate_ref, up_ref, out_refs)


def last_units(blocks_ref, before_ref, gain_ref, gate_ref, up_ref, stream_ref, *out_refs):
    stream = (before_ref[...].astype(f32) + jnp.sum(blocks_ref[...], axis=0)).astype(bf16)
    stream_ref[...] = stream
    send_units(stream, gain_ref, gate_ref, up_ref, out_refs)


def share_units(own_ref, one_ref, two_ref, three_ref, out_ref):
    total = in_pairs([ref[...].astype(f32) for ref in (own_ref, one_ref, two_ref, three_ref)])
    at = total.shape[0] - 8
    high, low = halves(jnp.sum(total[at:], axis=1, keepdims=True))
    lane = iota((8, LANES), 1)
    squares = jnp.where(lane == 0, high, jnp.where(lane == 1, low, 0.0)).astype(bf16)
    groups = out_ref.shape[0]
    out_ref[:, 0:at] = jnp.broadcast_to(total[0:at].astype(bf16)[None], (groups, at, LANES))
    out_ref[:, at:] = jnp.broadcast_to(squares[None], (groups, 8, LANES))


def gate_units(parts_ref, out_ref):
    total = jnp.sum(parts_ref[...].astype(f32), axis=0)
    at = total.shape[0] - 8
    squares = jnp.sum(total[at:], axis=1, keepdims=True)
    inv_rms = lax.rsqrt(squares / WIDTH + epsilon)
    upper = iota((8, LANES), 0) < 4
    tiles = at // 8

    def hidden(k, turned):
        scaled = total[k * 8 : k * 8 + 8] * inv_rms
        gated = jax.nn.silu(scaled)
        if turned:
            return pltpu.roll(gated, 4, 0) * scaled
        return gated * pltpu.roll(scaled, 4, 0)

    for k in range(0, tiles, 2):
        below = hidden(k + 1, True) if k + 1 < tiles else jnp.zeros((8, LANES), f32)
        out_ref[k * 4 : k * 4 + 8] = jnp.where(upper, hidden(k, False), below).astype(bf16)


def sum_down(own_ref, one_ref, two_ref, three_ref, down_ref, out_ref, part_ref):
    tiles = down_ref.shape[0] // LANES
    blocks = []
    for k in range(tiles):
        rows = slice(k // 2 * 8, k // 2 * 8 + 8)
        stacked = jnp.concatenate(
            [ref[rows].astype(f32) for ref in (own_ref, three_ref, two_ref, one_ref)], axis=0
        )
        mine = iota(stacked.shape, 0) % 8 // 4 == k % 2
        blocks.append(jnp.where(mine, stacked, 0.0).astype(bf16))
    part = matmul(jnp.concatenate(blocks, axis=1), down_ref[...])
    part_ref[0:32] = part
    part_ref[32:64] = part
    turn = lax.rem(4 - lax.axis_index("kv_1"), 4) * 8
    part = part_ref[pl.ds(pl.multiple_of(turn, 8), 32), :]
    part = part + pltpu.roll(part, 28, 0)
    part = jnp.concatenate([part[k * 8 : k * 8 + 4] for k in range(4)], axis=0)
    out_ref[...] = jnp.broadcast_to(part[None], out_ref.shape)


def turned(arrays, axis):
    devices = lax.axis_size(axis)
    return [arrays[0]] + [
        lax.ppermute(arrays[turn], axis, [(k, (k + turn) % devices) for k in range(devices)])
        for turn in range(1, devices)
    ]


def rotations(array, axis):
    return turned([array] * lax.axis_size(axis), axis)


def in_pairs(values):
    own, one, two, three = values
    return (own + two) + (one + three)


def as_row(column):
    size = column.shape[0]
    same = iota((size, LANES), 0) == iota((size, LANES), 1)
    return jnp.sum(jnp.where(same, column, 0.0), axis=0, keepdims=True)


def as_rows(parts):
    row = iota((8, LANES), 0)
    stacked = jnp.zeros((8, LANES), f32)
    for k, part in enumerate(parts):
        stacked = jnp.where(row == k, part, stacked)
    return stacked


def send_heads(
    blocks_ref, tokens_ref, gain_ref, query_ref, key_ref, value_ref, out_ref, stream_ref
):
    branch = jnp.sum(blocks_ref[...], axis=0)
    stream = (tokens_ref[...].astype(f32) + 0.5 * branch).astype(bf16)
    stream_ref[...] = stream
    wide = stream.astype(f32)
    squares = as_row(jnp.sum(wide * wide, axis=1, keepdims=True))
    scaled = (wide * gain_ref[...]).astype(bf16)
    at = 0
    for weight_ref in (query_ref, key_ref, value_ref):
        product = matmul(scaled, weight_ref[...]).astype(bf16)
        for h in range(product.shape[1] // LANES):
            out_ref[at : at + ROWS] = product[:, h * LANES : (h + 1) * LANES]
            at += ROWS
    out_ref[at:] = as_rows(halves(squares)).astype(bf16)


def share_heads(own_ref, one_ref, two_ref, three_ref, out_ref):
    total = in_pairs([ref[...].astype(f32) for ref in (own_ref, one_ref, two_ref, three_ref)])
    query = total[0:64].astype(bf16)
    fresh = total[64:192].astype(bf16)
    squares = total[192:193] + total[193:194]
    groups = out_ref.shape[0]
    row, col = iota((groups * 8, LANES), 0), iota((groups * 8, LANES), 1)
    part = row % 8
    place = row // 8 * lax.axis_size("kv_1") + lax.axis_index("kv_1")
    source = ((part // 2) * 4 + (place % 2) * 2 + part % 2) * ROWS + place // 2
    order = ((part < 4) & (col == source)).astype(bf16)
    fresh = matmul(order, fresh).reshape(groups, 8, LANES)
    high, low = halves(squares)
    fresh = fresh + as_rows([0.0] * 4 + [high, low])[None]
    out_ref[:, 0:64] = jnp.broadcast_to(query[None], (groups, 64, LANES))
    out_ref[:, 64:72] = fresh.astype(bf16)


def attend(
    lengths_ref, parts_ref, keys_ref, values_ref, out_ref, scores_ref, weights_ref, stats_ref
):
    total = jnp.sum(parts_ref[...].astype(f32), axis=0)
    squares = total[68:69] + total[69:70]
    token, lane = iota((ROWS, LANES), 0), iota((ROWS, LANES), 1)
    squares = jnp.sum(jnp.where(token == lane, squares, 0.0), axis=1, keepdims=True)
    inv_rms = lax.rsqrt(squares / WIDTH + epsilon)
    query = (total[0:64] * jnp.concatenate([inv_rms] * 4, axis=0)).astype(bf16)
    row, col = iota((LANES, 64), 0), iota((LANES, 64), 1)
    order = (col == (row % 8) // 2 * ROWS + row // 8).astype(bf16)
    query = matmul(order, query)
    row, lane = iota((LANES, LANES), 0), iota((LANES, LANES), 1)
    query = jnp.where(lane // HEAD_DIM == row % 2, query, 0.0)
    place = kv_index()
    own_inv = jnp.sum(
        jnp.where(iota((ROWS, 1), 0) == place // 2, inv_rms, 0.0), axis=0, keepdims=True
    )
    fresh = (total[64:72] * own_inv).astype(bf16)
    row, col = iota((LANES, 8), 0), iota((LANES, 8), 1)
    own_key = matmul((col == row % 4 // 2).astype(bf16), fresh)
    own_value = matmul((col == row % 4 // 2 + 2).astype(bf16), fresh)
    owned = iota((LANES, 1), 0) // 4 == place
    self_score = jnp.sum(query * own_key, axis=1, keepdims=True) * HEAD_DIM**-0.5
    self_score = jnp.where(owned, self_score, neg_fill)
    query = query.astype(bf16)
    columns = keys_ref.shape[1]
    offset = place * (columns // 4)
    col = iota((8, columns), 1)
    same_head = col % 4 == iota((8, columns), 0) // 2
    position = jnp.where(same_head, col // 4 + offset, 1 << 30)
    for b in range(ROWS):
        rows = slice(b * 8, b * 8 + 8)
        scores_ref[rows] = lax.dot_general(
            query[rows],
            keys_ref[b],
            (((1,), (1,)), ((), ())),
            preferred_element_type=f32,
        )
    for b in range(ROWS):
        rows = slice(b * 8, b * 8 + 8)
        live = position < lengths_ref[b]
        scores = jnp.where(live, scores_ref[rows] * HEAD_DIM**-0.5, neg_fill)
        peak = jnp.maximum(jnp.max(scores, axis=1, keepdims=True), self_score[rows])
        weights = jnp.where(live, jnp.exp(scores - peak), 0.0)
        own_weight = jnp.where(owned[rows], jnp.exp(self_score[rows] - peak), 0.0)
        amount = jnp.sum(weights, axis=1, keepdims=True) + own_weight
        weights_ref[rows] = weights.astype(bf16)
        stats_ref[0, rows] = jnp.broadcast_to(peak, (8, LANES))
        stats_ref[1, rows] = jnp.broadcast_to(amount, (8, LANES))
        stats_ref[2, rows] = own_weight.astype(bf16).astype(f32) * own_value[rows]
    for b in range(ROWS):
        rows = slice(b * 8, b * 8 + 8)
        weighted = matmul(weights_ref[rows], values_ref[b]) + stats_ref[2, rows]
        out_ref[rows] = weighted.astype(bf16)
    parts = thirds(as_row(stats_ref[0])) + thirds(as_row(stats_ref[1]))
    out_ref[LANES:] = as_rows(parts).astype(bf16)


def peak_and_amount(stats):
    stats = stats.astype(f32)
    return stats[0:1] + stats[1:2] + stats[2:3], stats[3:4] + stats[4:5] + stats[5:6]


def join(own_ref, one_ref, two_ref, three_ref, out_ref):
    refs = (own_ref, one_ref, two_ref, three_ref)
    peaks, amounts = zip(*[peak_and_amount(ref[LANES:]) for ref in refs])
    highest = functools.reduce(jnp.maximum, peaks)
    scales = [jnp.exp(peak - highest) for peak in peaks]
    amount = in_pairs([scale * amount for scale, amount in zip(scales, amounts)])
    scales = as_rows(scales).T
    weighted = in_pairs(
        [scales[:, k : k + 1] * ref[0:LANES].astype(f32) for k, ref in enumerate(refs)]
    )
    groups = out_ref.shape[0]
    stats = as_rows(thirds(highest) + thirds(amount)).astype(bf16)
    out_ref[:, 0:LANES] = jnp.broadcast_to(weighted.astype(bf16)[None], (groups, LANES, LANES))
    out_ref[:, LANES:] = jnp.broadcast_to(stats[None], (groups, 8, LANES))


def finish_heads(parts_ref, lam_ref, gain_ref, weight_ref, out_ref):
    groups = parts_ref.shape[0]
    peaks, amounts = zip(*[peak_and_amount(parts_ref[k, LANES:]) for k in range(groups)])
    highest = functools.reduce(jnp.maximum, peaks)
    scales = [jnp.exp(peak - highest) for peak in peaks]
    amount = sum(scale * amount for scale, amount in zip(scales, amounts))
    lane = iota((1, LANES), 1)
    share = jnp.ones((1, LANES), f32)
    for h in range(lam_ref.shape[1]):
        share = jnp.where(lane % 8 == 2 * h + 1, -lam_ref[:, h : h + 1], share)
    share = share / amount
    shares = as_rows([scale * share for scale in scales]).T
    ratio = sum(shares[:, k : k + 1] * parts_ref[k, 0:LANES].astype(f32) for k in range(groups))
    mixed = ratio + pltpu.roll(ratio, LANES - 1, 0)
    spread = jnp.mean(mixed * mixed, axis=1, keepdims=True)
    attended = (mixed * lax.rsqrt(spread + epsilon) * gain_ref[...]).astype(bf16)
    row, col = iota((64, LANES), 0), iota((64, LANES), 1)
    order = (col == (row % ROWS) * 8 + row // ROWS * 2).astype(bf16)
    attended = matmul(order, attended).astype(bf16)
    attended = jnp.concatenate(
        [attended[h * ROWS : (h + 1) * ROWS] for h in range(64 // ROWS)], axis=1
    )
    part = matmul(attended, weight_ref[...])
    out_ref[...] = jnp.broadcast_to(part[None], out_ref.shape)


def finish(blocks_ref, before_ref, out_ref):
    branch = jnp.sum(blocks_ref[...], axis=0)
    stream = (before_ref[...].astype(f32) + 0.5 * branch).astype(bf16)
    own = lax.dot_general(
        stream, own_columns(0), (((1,), (1,)), ((), ())), preferred_element_type=f32
    )
    out_ref[...] = own.astype(bf16)


def on_device(
    tokens,
    first_gain,
    first_gate,
    first_up,
    first_down,
    mixer_gain,
    w_query,
    w_key,
    w_value,
    w_output,
    lam_heads,
    head_gain,
    key_cache,
    value_cache,
    lengths,
    last_gain,
    last_gate,
    last_up,
    last_down,
):
    tp = lax.axis_size("tp")
    stream_like = like((ROWS, LANES), bf16)
    planes = lax.axis_size("kv_0")
    tiles = first_gate.shape[1] // LANES
    units_like = (stream_like,) + (like((tiles * 8 + 8, LANES), bf16),) * 4
    sums_like = like((tp, ROWS, LANES), f32)

    def hidden_sums(units, down_w):
        shared = in_kernel(
            share_units, like((planes, *units[0].shape), bf16), *turned(units, "kv_1")
        )
        hidden = in_kernel(
            gate_units, like(((tiles + 1) // 2 * 8, LANES), bf16), swap(shared, "kv_0")
        )
        sums = in_kernel(
            sum_down,
            sums_like,
            *rotations(hidden, "kv_1"),
            down_w,
            scratch=(pltpu.VMEM((64, LANES), f32),),
        )
        return swap(sums, "tp")

    blocks = swap(in_kernel(spread_tokens, like((tp, ROWS, LANES), bf16), tokens), "tp")
    stream, *units = in_kernel(
        first_units,
        units_like,
        blocks,
        first_gain.reshape(1, LANES),
        first_gate,
        first_up,
    )
    heads, first = in_kernel(
        send_heads,
        (like((200, LANES), bf16), stream_like),
        hidden_sums(units, first_down),
        stream,
        mixer_gain.reshape(1, LANES),
        w_query,
        w_key,
        w_value,
    )
    heads = in_kernel(share_heads, like((planes, 72, LANES), bf16), *rotations(heads, "kv_1"))
    rows, local, shard_heads, _ = key_cache.shape
    columns = local * shard_heads
    part = in_kernel(
        attend,
        like((LANES + 8, LANES), bf16),
        lengths,
        swap(heads, "kv_0"),
        key_cache.reshape(rows, columns, LANES),
        value_cache.reshape(rows, columns, LANES),
        smem=(0,),
        scratch=(
            pltpu.VMEM((LANES, columns), f32),
            pltpu.VMEM((LANES, columns), bf16),
            pltpu.VMEM((3, LANES, LANES), f32),
        ),
        vmem_limit=32 << 20,
    )
    parts = in_kernel(
        join, like((planes, LANES + 8, LANES), bf16), *rotations(part, "kv_1")
    )
    sums = in_kernel(
        finish_heads,
        sums_like,
        swap(parts, "kv_0"),
        lam_heads.reshape(1, shard_heads),
        head_gain.reshape(1, LANES),
        w_output,
    )
    sums = swap(sums, "tp")
    second, *units = in_kernel(
        last_units,
        units_like,
        sums,
        first,
        last_gain.reshape(1, LANES),
        last_gate,
        last_up,
    )
    return in_kernel(
        finish, like((ROWS, ROWS), bf16), hidden_sums(units, last_down), second
    )


def solution(mesh):
    finer = Mesh(mesh.devices.reshape(8, 4, mesh.shape["tp"]), ("kv_0", "kv_1", "tp"))
    return jax.shard_map(
        on_device,
        mesh=finer,
        in_specs=(
            P(None, KV_TP),
            P(KV),
            P(KV, "tp"),
            P(KV, "tp"),
            P("tp", KV),
            P(KV),
            P(KV, "tp"),
            P(KV, "tp"),
            P(KV, "tp"),
            P("tp", KV),
            P("tp"),
            P(),
            P(None, KV, "tp", None),
            P(None, KV, "tp", None),
            P(),
            P(KV),
            P(KV, "tp"),
            P(KV, "tp"),
            P("tp", KV),
        ),
        out_specs=P(None, KV_TP),
        check_vma=False,
    )
```

```python
import functools

import jax
import jax.numpy as jnp
from jax import lax
from jax.experimental import pallas as pl
from jax.experimental.pallas import tpu as pltpu
from jax.sharding import Mesh
from jax.sharding import PartitionSpec as P

WIDTH = 4096
ROWS = 16
HEAD_DIM = 64
LANES = 128
KV = ("kv_0", "kv_1")
KV_TP = ("kv_0", "kv_1", "tp")


epsilon = 1e-06
neg_fill = -1e30
f32 = jnp.float32
bf16 = jnp.bfloat16
covering = pl.CostEstimate(flops=10**10, bytes_accessed=10**5, transcendentals=0)


def iota(shape, dim):
    return lax.broadcasted_iota(jnp.int32, shape, dim)


def matmul(a, b):
    return jnp.dot(a, b, preferred_element_type=f32)


def in_kernel(body, outs, *args, smem=(), scratch=(), vmem_limit=16 << 20):
    spaces = [pltpu.SMEM if k in smem else pltpu.VMEM for k in range(len(args))]
    return pl.pallas_call(
        body,
        out_shape=outs,
        in_specs=[pl.BlockSpec(memory_space=space) for space in spaces],
        out_specs=jax.tree.map(lambda _: pl.BlockSpec(memory_space=pltpu.VMEM), outs),
        scratch_shapes=scratch,
        compiler_params=pltpu.CompilerParams(vmem_limit_bytes=vmem_limit),
        cost_estimate=covering,
        name=body.__name__,
    )(*args)


def swap(blocks, axis):
    return lax.all_to_all(blocks, axis, split_axis=0, concat_axis=0, tiled=True)


def like(shape, kind):
    return jax.ShapeDtypeStruct(shape, kind)


def kv_index():
    return lax.axis_index("kv_0") * lax.axis_size("kv_1") + lax.axis_index("kv_1")


def halves(column):
    high = column.astype(bf16)
    low = (column - high.astype(f32)).astype(bf16)
    return high.astype(f32), low.astype(f32)


def thirds(column):
    high, low = halves(column)
    rest = (column - high) - low
    return high, low, rest


def own_columns(shape_dim):
    place = lax.axis_index("tp") * ROWS
    return (iota((ROWS, LANES), 1) == iota((ROWS, LANES), 0) + place).astype(bf16)


def spread_tokens(tokens_ref, out_ref):
    block = matmul(tokens_ref[...], own_columns(0)).astype(bf16)
    out_ref[...] = jnp.broadcast_to(block[None], out_ref.shape)


def send_units(stream, gain_ref, gate_ref, up_ref, out_refs):
    groups = len(out_refs)
    size = ROWS // groups
    row, col = iota((groups * 8, ROWS), 0), iota((groups * 8, ROWS), 1)
    target = lax.rem(lax.axis_index("kv_1") + row // 8, groups)
    order = (col == target * size + row % size).astype(bf16)
    wide = matmul(order, stream)
    high, low = halves(jnp.sum(wide * wide, axis=1, keepdims=True))
    lane = iota((groups * 8, LANES), 1)
    squares = jnp.where(lane == 0, high, jnp.where(lane == 1, low, 0.0)).astype(bf16)
    scaled = (wide * gain_ref[...]).astype(bf16)
    gate = matmul(scaled, gate_ref[...])
    up = matmul(scaled, up_ref[...])
    both = jnp.where(iota(gate.shape, 0) % 8 < size, gate, up).astype(bf16)
    tiles = both.shape[1] // LANES
    for turn, out_ref in enumerate(out_refs):
        rows = slice(turn * 8, turn * 8 + 8)
        for k in range(tiles):
            out_ref[k * 8 : k * 8 + 8] = both[rows, k * LANES : (k + 1) * LANES]
        out_ref[tiles * 8 :] = squares[rows]


def first_units(blocks_ref, gain_ref, gate_ref, up_ref, stream_ref, *out_refs):
    stream = jnp.sum(blocks_ref[...].astype(f32), axis=0).astype(bf16)
    stream_ref[...] = stream
    send_units(stream, gain_ref, gate_ref, up_ref, out_refs)


def last_units(blocks_ref, before_ref, gain_ref, gate_ref, up_ref, stream_ref, *out_refs):
    stream = (before_ref[...].astype(f32) + jnp.sum(blocks_ref[...].astype(f32), axis=0)).astype(bf16)
    stream_ref[...] = stream
    send_units(stream, gain_ref, gate_ref, up_ref, out_refs)


def share_units(own_ref, one_ref, two_ref, three_ref, out_ref):
    total = in_pairs([ref[...].astype(f32) for ref in (own_ref, one_ref, two_ref, three_ref)])
    at = total.shape[0] - 8
    high, low = halves(jnp.sum(total[at:], axis=1, keepdims=True))
    lane = iota((8, LANES), 1)
    squares = jnp.where(lane == 0, high, jnp.where(lane == 1, low, 0.0)).astype(bf16)
    groups = out_ref.shape[0]
    out_ref[:, 0:at] = jnp.broadcast_to(total[0:at].astype(bf16)[None], (groups, at, LANES))
    out_ref[:, at:] = jnp.broadcast_to(squares[None], (groups, 8, LANES))


def gate_units(parts_ref, out_ref):
    total = jnp.sum(parts_ref[...].astype(f32), axis=0)
    at = total.shape[0] - 8
    squares = jnp.sum(total[at:], axis=1, keepdims=True)
    inv_rms = lax.rsqrt(squares / WIDTH + epsilon)
    upper = iota((8, LANES), 0) < 4
    tiles = at // 8

    def hidden(k, turned):
        scaled = total[k * 8 : k * 8 + 8] * inv_rms
        gated = jax.nn.silu(scaled)
        if turned:
            return pltpu.roll(gated, 4, 0) * scaled
        return gated * pltpu.roll(scaled, 4, 0)

    for k in range(0, tiles, 2):
        below = hidden(k + 1, True) if k + 1 < tiles else jnp.zeros((8, LANES), f32)
        out_ref[k * 4 : k * 4 + 8] = jnp.where(upper, hidden(k, False), below).astype(bf16)


def sum_down(own_ref, one_ref, two_ref, three_ref, down_ref, out_ref, part_ref):
    tiles = down_ref.shape[0] // LANES
    blocks = []
    for k in range(tiles):
        rows = slice(k // 2 * 8, k // 2 * 8 + 8)
        stacked = jnp.concatenate(
            [ref[rows].astype(f32) for ref in (own_ref, three_ref, two_ref, one_ref)], axis=0
        )
        mine = iota(stacked.shape, 0) % 8 // 4 == k % 2
        blocks.append(jnp.where(mine, stacked, 0.0).astype(bf16))
    part = matmul(jnp.concatenate(blocks, axis=1), down_ref[...])
    part_ref[0:32] = part
    part_ref[32:64] = part
    turn = lax.rem(4 - lax.axis_index("kv_1"), 4) * 8
    part = part_ref[pl.ds(pl.multiple_of(turn, 8), 32), :]
    part = part + pltpu.roll(part, 28, 0)
    part = jnp.concatenate([part[k * 8 : k * 8 + 4] for k in range(4)], axis=0)
    out_ref[...] = jnp.broadcast_to(part.astype(bf16)[None], out_ref.shape)


def turned(arrays, axis):
    devices = lax.axis_size(axis)
    return [arrays[0]] + [
        lax.ppermute(arrays[turn], axis, [(k, (k + turn) % devices) for k in range(devices)])
        for turn in range(1, devices)
    ]


def rotations(array, axis):
    return turned([array] * lax.axis_size(axis), axis)


def in_pairs(values):
    own, one, two, three = values
    return (own + two) + (one + three)


def as_row(column):
    size = column.shape[0]
    same = iota((size, LANES), 0) == iota((size, LANES), 1)
    return jnp.sum(jnp.where(same, column, 0.0), axis=0, keepdims=True)


def as_rows(parts):
    row = iota((8, LANES), 0)
    stacked = jnp.zeros((8, LANES), f32)
    for k, part in enumerate(parts):
        stacked = jnp.where(row == k, part, stacked)
    return stacked


def send_heads(
    blocks_ref, tokens_ref, gain_ref, query_ref, key_ref, value_ref, out_ref, stream_ref
):
    branch = jnp.sum(blocks_ref[...].astype(f32), axis=0)
    stream = (tokens_ref[...].astype(f32) + 0.5 * branch).astype(bf16)
    stream_ref[...] = stream
    wide = stream.astype(f32)
    squares = as_row(jnp.sum(wide * wide, axis=1, keepdims=True))
    scaled = (wide * gain_ref[...]).astype(bf16)
    at = 0
    for weight_ref in (query_ref, key_ref, value_ref):
        product = matmul(scaled, weight_ref[...]).astype(bf16)
        for h in range(product.shape[1] // LANES):
            out_ref[at : at + ROWS] = product[:, h * LANES : (h + 1) * LANES]
            at += ROWS
    out_ref[at:] = as_rows(halves(squares)).astype(bf16)


def share_heads(own_ref, one_ref, two_ref, three_ref, out_ref):
    total = in_pairs([ref[...].astype(f32) for ref in (own_ref, one_ref, two_ref, three_ref)])
    query = total[0:64].astype(bf16)
    fresh = total[64:192].astype(bf16)
    squares = total[192:193] + total[193:194]
    groups = out_ref.shape[0]
    row, col = iota((groups * 8, LANES), 0), iota((groups * 8, LANES), 1)
    part = row % 8
    place = row // 8 * lax.axis_size("kv_1") + lax.axis_index("kv_1")
    source = ((part // 2) * 4 + (place % 2) * 2 + part % 2) * ROWS + place // 2
    order = ((part < 4) & (col == source)).astype(bf16)
    fresh = matmul(order, fresh).reshape(groups, 8, LANES)
    high, low = halves(squares)
    fresh = fresh + as_rows([0.0] * 4 + [high, low])[None]
    out_ref[:, 0:64] = jnp.broadcast_to(query[None], (groups, 64, LANES))
    out_ref[:, 64:72] = fresh.astype(bf16)


def attend(
    lengths_ref, parts_ref, keys_ref, values_ref, out_ref, scores_ref, weights_ref, stats_ref
):
    total = jnp.sum(parts_ref[...].astype(f32), axis=0)
    squares = total[68:69] + total[69:70]
    token, lane = iota((ROWS, LANES), 0), iota((ROWS, LANES), 1)
    squares = jnp.sum(jnp.where(token == lane, squares, 0.0), axis=1, keepdims=True)
    inv_rms = lax.rsqrt(squares / WIDTH + epsilon)
    query = (total[0:64] * jnp.concatenate([inv_rms] * 4, axis=0)).astype(bf16)
    row, col = iota((LANES, 64), 0), iota((LANES, 64), 1)
    order = (col == (row % 8) // 2 * ROWS + row // 8).astype(bf16)
    query = matmul(order, query)
    row, lane = iota((LANES, LANES), 0), iota((LANES, LANES), 1)
    query = jnp.where(lane // HEAD_DIM == row % 2, query, 0.0)
    place = kv_index()
    own_inv = jnp.sum(
        jnp.where(iota((ROWS, 1), 0) == place // 2, inv_rms, 0.0), axis=0, keepdims=True
    )
    fresh = (total[64:72] * own_inv).astype(bf16)
    row, col = iota((LANES, 8), 0), iota((LANES, 8), 1)
    own_key = matmul((col == row % 4 // 2).astype(bf16), fresh)
    own_value = matmul((col == row % 4 // 2 + 2).astype(bf16), fresh)
    owned = iota((LANES, 1), 0) // 4 == place
    self_score = jnp.sum(query * own_key, axis=1, keepdims=True) * HEAD_DIM**-0.5
    self_score = jnp.where(owned, self_score, neg_fill)
    query = query.astype(bf16)
    columns = keys_ref.shape[1]
    offset = place * (columns // 4)
    col = iota((8, columns), 1)
    same_head = col % 4 == iota((8, columns), 0) // 2
    position = jnp.where(same_head, col // 4 + offset, 1 << 30)
    for b in range(ROWS):
        rows = slice(b * 8, b * 8 + 8)
        scores_ref[rows] = lax.dot_general(
            query[rows],
            keys_ref[b],
            (((1,), (1,)), ((), ())),
            preferred_element_type=f32,
        )
    for b in range(ROWS):
        rows = slice(b * 8, b * 8 + 8)
        live = position < lengths_ref[b]
        scores = jnp.where(live, scores_ref[rows] * HEAD_DIM**-0.5, neg_fill)
        peak = jnp.maximum(jnp.max(scores, axis=1, keepdims=True), self_score[rows])
        weights = jnp.where(live, jnp.exp(scores - peak), 0.0)
        own_weight = jnp.where(owned[rows], jnp.exp(self_score[rows] - peak), 0.0)
        amount = jnp.sum(weights, axis=1, keepdims=True) + own_weight
        weights_ref[rows] = weights.astype(bf16)
        stats_ref[0, rows] = jnp.broadcast_to(peak, (8, LANES))
        stats_ref[1, rows] = jnp.broadcast_to(amount, (8, LANES))
        stats_ref[2, rows] = own_weight.astype(bf16).astype(f32) * own_value[rows]
    for b in range(ROWS):
        rows = slice(b * 8, b * 8 + 8)
        scores_ref[rows, 0:LANES] = matmul(weights_ref[rows], values_ref[b]) + stats_ref[2, rows]
    out_ref[0:LANES] = scores_ref[:, 0:LANES].T.astype(bf16)
    parts = thirds(as_row(stats_ref[0])) + thirds(as_row(stats_ref[1]))
    out_ref[LANES:] = as_rows(parts).astype(bf16)


def peak_and_amount(stats):
    stats = stats.astype(f32)
    return stats[0:1] + stats[1:2] + stats[2:3], stats[3:4] + stats[4:5] + stats[5:6]


def join(own_ref, one_ref, two_ref, three_ref, out_ref):
    refs = (own_ref, one_ref, two_ref, three_ref)
    peaks, amounts = zip(*[peak_and_amount(ref[LANES:]) for ref in refs])
    highest = functools.reduce(jnp.maximum, peaks)
    scales = [jnp.exp(peak - highest) for peak in peaks]
    amount = in_pairs([scale * amount for scale, amount in zip(scales, amounts)])
    weighted = in_pairs([scale * ref[0:LANES].astype(f32) for scale, ref in zip(scales, refs)])
    groups = out_ref.shape[0]
    stats = as_rows(thirds(highest) + thirds(amount)).astype(bf16)
    out_ref[:, 0:LANES] = jnp.broadcast_to(weighted.astype(bf16)[None], (groups, LANES, LANES))
    out_ref[:, LANES:] = jnp.broadcast_to(stats[None], (groups, 8, LANES))


def finish_heads(parts_ref, lam_ref, gain_ref, weight_ref, out_ref):
    groups = parts_ref.shape[0]
    peaks, amounts = zip(*[peak_and_amount(parts_ref[k, LANES:]) for k in range(groups)])
    highest = functools.reduce(jnp.maximum, peaks)
    scales = [jnp.exp(peak - highest) for peak in peaks]
    amount = sum(scale * amount for scale, amount in zip(scales, amounts))
    lane = iota((1, LANES), 1)
    share = jnp.ones((1, LANES), f32)
    for h in range(lam_ref.shape[1]):
        share = jnp.where(lane % 8 == 2 * h + 1, -lam_ref[:, h : h + 1], share)
    share = share / amount
    ratio = sum(
        scale * share * parts_ref[k, 0:LANES].astype(f32) for k, scale in enumerate(scales)
    )
    mixed = ratio + pltpu.roll(ratio, LANES - 1, 1)
    spread = jnp.mean(mixed * mixed, axis=0, keepdims=True)
    gain = jnp.broadcast_to(gain_ref[...], (8, LANES)).T[:, 0:1]
    attended = (mixed * lax.rsqrt(spread + epsilon) * gain).astype(bf16)
    row, col = iota((64, LANES), 0), iota((64, LANES), 1)
    order = (col == (row % ROWS) * 8 + row // ROWS * 2).astype(bf16)
    attended = lax.dot_general(
        order, attended, (((1,), (1,)), ((), ())), preferred_element_type=f32
    ).astype(bf16)
    attended = jnp.concatenate(
        [attended[h * ROWS : (h + 1) * ROWS] for h in range(64 // ROWS)], axis=1
    )
    part = matmul(attended, weight_ref[...])
    out_ref[...] = jnp.broadcast_to(part.astype(bf16)[None], out_ref.shape)


def finish(blocks_ref, before_ref, out_ref):
    branch = jnp.sum(blocks_ref[...].astype(f32), axis=0)
    stream = (before_ref[...].astype(f32) + 0.5 * branch).astype(bf16)
    own = lax.dot_general(
        stream, own_columns(0), (((1,), (1,)), ((), ())), preferred_element_type=f32
    )
    out_ref[...] = own.astype(bf16)


def on_device(
    tokens,
    first_gain,
    first_gate,
    first_up,
    first_down,
    mixer_gain,
    w_query,
    w_key,
    w_value,
    w_output,
    lam_heads,
    head_gain,
    key_cache,
    value_cache,
    lengths,
    last_gain,
    last_gate,
    last_up,
    last_down,
):
    tp = lax.axis_size("tp")
    stream_like = like((ROWS, LANES), bf16)
    planes = lax.axis_size("kv_0")
    tiles = first_gate.shape[1] // LANES
    units_like = (stream_like,) + (like((tiles * 8 + 8, LANES), bf16),) * 4
    sums_like = like((tp, ROWS, LANES), bf16)

    def hidden_sums(units, down_w):
        shared = in_kernel(
            share_units, like((planes, *units[0].shape), bf16), *turned(units, "kv_1")
        )
        hidden = in_kernel(
            gate_units, like(((tiles + 1) // 2 * 8, LANES), bf16), swap(shared, "kv_0")
        )
        sums = in_kernel(
            sum_down,
            sums_like,
            *rotations(hidden, "kv_1"),
            down_w,
            scratch=(pltpu.VMEM((64, LANES), f32),),
        )
        return swap(sums, "tp")

    blocks = swap(in_kernel(spread_tokens, like((tp, ROWS, LANES), bf16), tokens), "tp")
    stream, *units = in_kernel(
        first_units,
        units_like,
        blocks,
        first_gain.reshape(1, LANES),
        first_gate,
        first_up,
    )
    heads, first = in_kernel(
        send_heads,
        (like((200, LANES), bf16), stream_like),
        hidden_sums(units, first_down),
        stream,
        mixer_gain.reshape(1, LANES),
        w_query,
        w_key,
        w_value,
    )
    heads = in_kernel(share_heads, like((planes, 72, LANES), bf16), *rotations(heads, "kv_1"))
    rows, local, shard_heads, _ = key_cache.shape
    columns = local * shard_heads
    part = in_kernel(
        attend,
        like((LANES + 8, LANES), bf16),
        lengths,
        swap(heads, "kv_0"),
        key_cache.reshape(rows, columns, LANES),
        value_cache.reshape(rows, columns, LANES),
        smem=(0,),
        scratch=(
            pltpu.VMEM((LANES, columns), f32),
            pltpu.VMEM((LANES, columns), bf16),
            pltpu.VMEM((3, LANES, LANES), f32),
        ),
        vmem_limit=32 << 20,
    )
    parts = in_kernel(
        join, like((planes, LANES + 8, LANES), bf16), *rotations(part, "kv_1")
    )
    sums = in_kernel(
        finish_heads,
        sums_like,
        swap(parts, "kv_0"),
        lam_heads.reshape(1, shard_heads),
        head_gain.reshape(1, LANES),
        w_output,
    )
    sums = swap(sums, "tp")
    second, *units = in_kernel(
        last_units,
        units_like,
        sums,
        first,
        last_gain.reshape(1, LANES),
        last_gate,
        last_up,
    )
    return in_kernel(
        finish, like((ROWS, ROWS), bf16), hidden_sums(units, last_down), second
    )


def solution(mesh):
    finer = Mesh(mesh.devices.reshape(8, 4, mesh.shape["tp"]), ("kv_0", "kv_1", "tp"))
    return jax.shard_map(
        on_device,
        mesh=finer,
        in_specs=(
            P(None, KV_TP),
            P(KV),
            P(KV, "tp"),
            P(KV, "tp"),
            P("tp", KV),
            P(KV),
            P(KV, "tp"),
            P(KV, "tp"),
            P(KV, "tp"),
            P("tp", KV),
            P("tp"),
            P(),
            P(None, KV, "tp", None),
            P(None, KV, "tp", None),
            P(),
            P(KV),
            P(KV, "tp"),
            P(KV, "tp"),
            P("tp", KV),
        ),
        out_specs=P(None, KV_TP),
        check_vma=False,
    )
```

```python
import functools

import jax
import jax.numpy as jnp
from jax import lax
from jax.experimental import pallas as pl
from jax.experimental.pallas import tpu as pltpu
from jax.sharding import Mesh
from jax.sharding import PartitionSpec as P

WIDTH = 4096
ROWS = 16
HEAD_DIM = 64
LANES = 128
KV = ("kv_0", "kv_1")
KV_TP = ("kv_0", "kv_1", "tp")


epsilon = 1e-06
neg_fill = -1e30
f32 = jnp.float32
bf16 = jnp.bfloat16
covering = pl.CostEstimate(flops=10**10, bytes_accessed=10**5, transcendentals=0)


def iota(shape, dim):
    return lax.broadcasted_iota(jnp.int32, shape, dim)


def matmul(a, b):
    return jnp.dot(a, b, preferred_element_type=f32)


def in_kernel(body, outs, *args, smem=(), scratch=(), vmem_limit=16 << 20):
    spaces = [pltpu.SMEM if k in smem else pltpu.VMEM for k in range(len(args))]
    return pl.pallas_call(
        body,
        out_shape=outs,
        in_specs=[pl.BlockSpec(memory_space=space) for space in spaces],
        out_specs=jax.tree.map(lambda _: pl.BlockSpec(memory_space=pltpu.VMEM), outs),
        scratch_shapes=scratch,
        compiler_params=pltpu.CompilerParams(vmem_limit_bytes=vmem_limit),
        cost_estimate=covering,
    )(*args)


def swap(blocks, axis):
    return lax.all_to_all(blocks, axis, split_axis=0, concat_axis=0, tiled=True)


def like(shape, kind):
    return jax.ShapeDtypeStruct(shape, kind)


def kv_index():
    return lax.axis_index("kv_0") * lax.axis_size("kv_1") + lax.axis_index("kv_1")


def halves(column):
    high = column.astype(bf16)
    low = (column - high.astype(f32)).astype(bf16)
    return high.astype(f32), low.astype(f32)


def thirds(column):
    high, low = halves(column)
    rest = (column - high) - low
    return high, low, rest


def own_columns():
    place = lax.axis_index("tp") * ROWS
    return (iota((ROWS, LANES), 1) == iota((ROWS, LANES), 0) + place).astype(bf16)


def spread_tokens(tokens_ref, out_ref):
    block = matmul(tokens_ref[...], own_columns()).astype(bf16)
    out_ref[...] = jnp.broadcast_to(block[None], out_ref.shape)


def send_units(stream, gain_ref, gate_ref, up_ref, out_refs):
    groups = len(out_refs)
    size = ROWS // groups
    row, col = iota((groups * 8, ROWS), 0), iota((groups * 8, ROWS), 1)
    target = lax.rem(lax.axis_index("kv_1") + row // 8, groups)
    order = (col == target * size + row % size).astype(bf16)
    wide = matmul(order, stream)
    high, low = halves(jnp.sum(wide * wide, axis=1, keepdims=True))
    lane = iota((groups * 8, LANES), 1)
    squares = jnp.where(lane == 0, high, jnp.where(lane == 1, low, 0.0)).astype(bf16)
    scaled = (wide * gain_ref[...]).astype(bf16)
    gate = matmul(scaled, gate_ref[...])
    up = matmul(scaled, up_ref[...])
    both = jnp.where(iota(gate.shape, 0) % 8 < size, gate, up).astype(bf16)
    tiles = both.shape[1] // LANES
    for turn, out_ref in enumerate(out_refs):
        rows = slice(turn * 8, turn * 8 + 8)
        for k in range(tiles):
            out_ref[k * 8 : k * 8 + 8] = both[rows, k * LANES : (k + 1) * LANES]
        out_ref[tiles * 8 :] = squares[rows]


def first_units(blocks_ref, gain_ref, gate_ref, up_ref, stream_ref, *out_refs):
    stream = jnp.sum(blocks_ref[...].astype(f32), axis=0).astype(bf16)
    stream_ref[...] = stream
    send_units(stream, gain_ref, gate_ref, up_ref, out_refs)


def last_units(blocks_ref, before_ref, gain_ref, gate_ref, up_ref, stream_ref, *out_refs):
    stream = (before_ref[...].astype(f32) + jnp.sum(blocks_ref[...].astype(f32), axis=0)).astype(bf16)
    stream_ref[...] = stream
    send_units(stream, gain_ref, gate_ref, up_ref, out_refs)


def share_units(own_ref, one_ref, two_ref, three_ref, out_ref):
    total = in_pairs([ref[...].astype(f32) for ref in (own_ref, one_ref, two_ref, three_ref)])
    at = total.shape[0] - 8
    high, low = halves(jnp.sum(total[at:], axis=1, keepdims=True))
    lane = iota((8, LANES), 1)
    squares = jnp.where(lane == 0, high, jnp.where(lane == 1, low, 0.0)).astype(bf16)
    groups = out_ref.shape[0]
    out_ref[:, 0:at] = jnp.broadcast_to(total[0:at].astype(bf16)[None], (groups, at, LANES))
    out_ref[:, at:] = jnp.broadcast_to(squares[None], (groups, 8, LANES))


def gate_units(parts_ref, out_ref):
    total = jnp.sum(parts_ref[...].astype(f32), axis=0)
    at = total.shape[0] - 8
    squares = jnp.sum(total[at:], axis=1, keepdims=True)
    inv_rms = lax.rsqrt(squares / WIDTH + epsilon)
    upper = iota((8, LANES), 0) < 4
    tiles = at // 8

    def hidden(k, turned):
        scaled = total[k * 8 : k * 8 + 8] * inv_rms
        gated = jax.nn.silu(scaled)
        if turned:
            return pltpu.roll(gated, 4, 0) * scaled
        return gated * pltpu.roll(scaled, 4, 0)

    for k in range(0, tiles, 2):
        below = hidden(k + 1, True) if k + 1 < tiles else jnp.zeros((8, LANES), f32)
        out_ref[k * 4 : k * 4 + 8] = jnp.where(upper, hidden(k, False), below).astype(bf16)


def sum_down(own_ref, one_ref, two_ref, three_ref, down_ref, out_ref, part_ref):
    tiles = down_ref.shape[0] // LANES
    blocks = []
    for k in range(tiles):
        rows = slice(k // 2 * 8, k // 2 * 8 + 8)
        stacked = jnp.concatenate(
            [ref[rows].astype(f32) for ref in (own_ref, three_ref, two_ref, one_ref)], axis=0
        )
        mine = iota(stacked.shape, 0) % 8 // 4 == k % 2
        blocks.append(jnp.where(mine, stacked, 0.0).astype(bf16))
    part = matmul(jnp.concatenate(blocks, axis=1), down_ref[...])
    part_ref[0:32] = part
    part_ref[32:64] = part
    turn = lax.rem(4 - lax.axis_index("kv_1"), 4) * 8
    part = part_ref[pl.ds(pl.multiple_of(turn, 8), 32), :]
    part = part + pltpu.roll(part, 28, 0)
    part = jnp.concatenate([part[k * 8 : k * 8 + 4] for k in range(4)], axis=0)
    out_ref[...] = jnp.broadcast_to(part.astype(bf16)[None], out_ref.shape)


def turned(arrays, axis):
    devices = lax.axis_size(axis)
    arrived = [arrays[0]]
    for turn in range(1, devices):
        pairs = [(k, (k + turn) % devices) for k in range(devices)]
        arrived.append(lax.ppermute(arrays[turn], axis, pairs))
    return arrived


def rotations(array, axis):
    return turned([array] * lax.axis_size(axis), axis)


def in_pairs(values):
    own, one, two, three = values
    return (own + two) + (one + three)


def as_row(column):
    size = column.shape[0]
    same = iota((size, LANES), 0) == iota((size, LANES), 1)
    return jnp.sum(jnp.where(same, column, 0.0), axis=0, keepdims=True)


def as_rows(parts):
    row = iota((8, LANES), 0)
    stacked = jnp.zeros((8, LANES), f32)
    for k, part in enumerate(parts):
        stacked = jnp.where(row == k, part, stacked)
    return stacked


def send_heads(
    blocks_ref, tokens_ref, gain_ref, query_ref, key_ref, value_ref, out_ref, stream_ref
):
    branch = jnp.sum(blocks_ref[...].astype(f32), axis=0)
    stream = (tokens_ref[...].astype(f32) + 0.5 * branch).astype(bf16)
    stream_ref[...] = stream
    wide = stream.astype(f32)
    squares = as_row(jnp.sum(wide * wide, axis=1, keepdims=True))
    scaled = (wide * gain_ref[...]).astype(bf16)
    at = 0
    for weight_ref in (query_ref, key_ref, value_ref):
        product = matmul(scaled, weight_ref[...]).astype(bf16)
        for h in range(product.shape[1] // LANES):
            out_ref[at : at + ROWS] = product[:, h * LANES : (h + 1) * LANES]
            at += ROWS
    out_ref[at:] = as_rows(halves(squares)).astype(bf16)


def share_heads(own_ref, one_ref, two_ref, three_ref, out_ref):
    total = in_pairs([ref[...].astype(f32) for ref in (own_ref, one_ref, two_ref, three_ref)])
    query = total[0:64].astype(bf16)
    fresh = total[64:192].astype(bf16)
    squares = total[192:193] + total[193:194]
    groups = out_ref.shape[0]
    row, col = iota((groups * 8, LANES), 0), iota((groups * 8, LANES), 1)
    part = row % 8
    place = row // 8 * lax.axis_size("kv_1") + lax.axis_index("kv_1")
    source = ((part // 2) * 4 + (place % 2) * 2 + part % 2) * ROWS + place // 2
    order = ((part < 4) & (col == source)).astype(bf16)
    fresh = matmul(order, fresh).reshape(groups, 8, LANES)
    high, low = halves(squares)
    fresh = fresh + as_rows([0.0] * 4 + [high, low])[None]
    out_ref[:, 0:64] = jnp.broadcast_to(query[None], (groups, 64, LANES))
    out_ref[:, 64:72] = fresh.astype(bf16)


def attend(
    lengths_ref, parts_ref, keys_ref, values_ref, out_ref, scores_ref, weights_ref, stats_ref
):
    total = jnp.sum(parts_ref[...].astype(f32), axis=0)
    squares = total[68:69] + total[69:70]
    token, lane = iota((ROWS, LANES), 0), iota((ROWS, LANES), 1)
    squares = jnp.sum(jnp.where(token == lane, squares, 0.0), axis=1, keepdims=True)
    inv_rms = lax.rsqrt(squares / WIDTH + epsilon)
    query = (total[0:64] * jnp.concatenate([inv_rms] * 4, axis=0)).astype(bf16)
    row, col = iota((LANES, 64), 0), iota((LANES, 64), 1)
    order = (col == (row % 8) // 2 * ROWS + row // 8).astype(bf16)
    query = matmul(order, query)
    row, lane = iota((LANES, LANES), 0), iota((LANES, LANES), 1)
    query = jnp.where(lane // HEAD_DIM == row % 2, query, 0.0)
    place = kv_index()
    rounded = query.astype(bf16)
    columns = keys_ref.shape[1]
    offset = place * (columns // 4)
    col = iota((8, columns), 1)
    same_head = col % 4 == iota((8, columns), 0) // 2
    position = jnp.where(same_head, col // 4 + offset, 1 << 30)
    for b in range(ROWS):
        rows = slice(b * 8, b * 8 + 8)
        scores_ref[rows] = lax.dot_general(
            rounded[rows],
            keys_ref[b],
            (((1,), (1,)), ((), ())),
            preferred_element_type=f32,
        )
    own_inv = jnp.sum(
        jnp.where(iota((ROWS, 1), 0) == place // 2, inv_rms, 0.0), axis=0, keepdims=True
    )
    fresh = (total[64:72] * own_inv).astype(bf16)
    row, col = iota((LANES, 8), 0), iota((LANES, 8), 1)
    own_key = matmul((col == row % 4 // 2).astype(bf16), fresh)
    own_value = matmul((col == row % 4 // 2 + 2).astype(bf16), fresh)
    owned = iota((LANES, 1), 0) // 4 == place
    self_score = jnp.sum(query * own_key, axis=1, keepdims=True) * HEAD_DIM**-0.5
    self_score = jnp.where(owned, self_score, neg_fill)
    for b in range(ROWS):
        rows = slice(b * 8, b * 8 + 8)
        live = position < lengths_ref[b]
        scores = jnp.where(live, scores_ref[rows] * HEAD_DIM**-0.5, neg_fill)
        peak = jnp.maximum(jnp.max(scores, axis=1, keepdims=True), self_score[rows])
        weights = jnp.where(live, jnp.exp(scores - peak), 0.0)
        own_weight = jnp.where(owned[rows], jnp.exp(self_score[rows] - peak), 0.0)
        amount = jnp.sum(weights, axis=1, keepdims=True) + own_weight
        weights_ref[rows] = weights.astype(bf16)
        stats_ref[0, rows] = jnp.broadcast_to(peak, (8, LANES))
        stats_ref[1, rows] = jnp.broadcast_to(amount, (8, LANES))
        stats_ref[2, rows] = own_weight.astype(bf16).astype(f32) * own_value[rows]
    for b in range(ROWS):
        rows = slice(b * 8, b * 8 + 8)
        scores_ref[rows, 0:LANES] = matmul(weights_ref[rows], values_ref[b]) + stats_ref[2, rows]
    out_ref[0:LANES] = scores_ref[:, 0:LANES].T.astype(bf16)
    parts = thirds(as_row(stats_ref[0])) + thirds(as_row(stats_ref[1]))
    out_ref[LANES:] = as_rows(parts).astype(bf16)


def peak_and_amount(stats):
    stats = stats.astype(f32)
    return stats[0:1] + stats[1:2] + stats[2:3], stats[3:4] + stats[4:5] + stats[5:6]


def join(own_ref, one_ref, two_ref, three_ref, out_ref):
    refs = (own_ref, one_ref, two_ref, three_ref)
    peaks, amounts = zip(*[peak_and_amount(ref[LANES:]) for ref in refs])
    highest = functools.reduce(jnp.maximum, peaks)
    scales = [jnp.exp(peak - highest) for peak in peaks]
    amount = in_pairs([scale * amount for scale, amount in zip(scales, amounts)])
    weighted = in_pairs([scale * ref[0:LANES].astype(f32) for scale, ref in zip(scales, refs)])
    groups = out_ref.shape[0]
    stats = as_rows(thirds(highest) + thirds(amount)).astype(bf16)
    out_ref[:, 0:LANES] = jnp.broadcast_to(weighted.astype(bf16)[None], (groups, LANES, LANES))
    out_ref[:, LANES:] = jnp.broadcast_to(stats[None], (groups, 8, LANES))


def finish_heads(parts_ref, lam_ref, gain_ref, weight_ref, out_ref):
    groups = parts_ref.shape[0]
    peaks, amounts = zip(*[peak_and_amount(parts_ref[k, LANES:]) for k in range(groups)])
    highest = functools.reduce(jnp.maximum, peaks)
    scales = [jnp.exp(peak - highest) for peak in peaks]
    amount = sum(scale * amount for scale, amount in zip(scales, amounts))
    lane = iota((1, LANES), 1)
    share = jnp.ones((1, LANES), f32)
    for h in range(lam_ref.shape[1]):
        share = jnp.where(lane % 8 == 2 * h + 1, -lam_ref[:, h : h + 1], share)
    share = share / amount
    ratio = sum(
        scale * share * parts_ref[k, 0:LANES].astype(f32) for k, scale in enumerate(scales)
    )
    mixed = ratio + pltpu.roll(ratio, LANES - 1, 1)
    spread = jnp.mean(mixed * mixed, axis=0, keepdims=True)
    gain = jnp.broadcast_to(gain_ref[...], (8, LANES)).T[:, 0:1]
    attended = (mixed * lax.rsqrt(spread + epsilon) * gain).astype(bf16)
    row, col = iota((64, LANES), 0), iota((64, LANES), 1)
    order = (col == (row % ROWS) * 8 + row // ROWS * 2).astype(bf16)
    attended = lax.dot_general(
        order, attended, (((1,), (1,)), ((), ())), preferred_element_type=f32
    ).astype(bf16)
    attended = jnp.concatenate(
        [attended[h * ROWS : (h + 1) * ROWS] for h in range(64 // ROWS)], axis=1
    )
    part = matmul(attended, weight_ref[...])
    out_ref[...] = jnp.broadcast_to(part.astype(bf16)[None], out_ref.shape)


def finish(blocks_ref, before_ref, out_ref):
    branch = jnp.sum(blocks_ref[...].astype(f32), axis=0)
    stream = (before_ref[...].astype(f32) + 0.5 * branch).astype(bf16)
    own = lax.dot_general(
        stream, own_columns(), (((1,), (1,)), ((), ())), preferred_element_type=f32
    )
    out_ref[...] = own.astype(bf16)


def on_device(
    tokens,
    first_gain,
    first_gate,
    first_up,
    first_down,
    mixer_gain,
    w_query,
    w_key,
    w_value,
    w_output,
    lam_heads,
    head_gain,
    key_cache,
    value_cache,
    lengths,
    last_gain,
    last_gate,
    last_up,
    last_down,
):
    tp = lax.axis_size("tp")
    stream_like = like((ROWS, LANES), bf16)
    planes = lax.axis_size("kv_0")
    tiles = first_gate.shape[1] // LANES
    units_like = (stream_like,) + (like((tiles * 8 + 8, LANES), bf16),) * 4
    sums_like = like((tp, ROWS, LANES), bf16)

    def hidden_sums(units, down_w):
        shared = in_kernel(
            share_units, like((planes, *units[0].shape), bf16), *turned(units, "kv_1")
        )
        hidden = in_kernel(
            gate_units, like(((tiles + 1) // 2 * 8, LANES), bf16), swap(shared, "kv_0")
        )
        sums = in_kernel(
            sum_down,
            sums_like,
            *rotations(hidden, "kv_1"),
            down_w,
            scratch=(pltpu.VMEM((64, LANES), f32),),
        )
        return swap(sums, "tp")

    blocks = swap(in_kernel(spread_tokens, like((tp, ROWS, LANES), bf16), tokens), "tp")
    stream, *units = in_kernel(
        first_units,
        units_like,
        blocks,
        first_gain.reshape(1, LANES),
        first_gate,
        first_up,
    )
    heads, first = in_kernel(
        send_heads,
        (like((200, LANES), bf16), stream_like),
        hidden_sums(units, first_down),
        stream,
        mixer_gain.reshape(1, LANES),
        w_query,
        w_key,
        w_value,
    )
    heads = in_kernel(share_heads, like((planes, 72, LANES), bf16), *rotations(heads, "kv_1"))
    rows, local, shard_heads, _ = key_cache.shape
    columns = local * shard_heads
    part = in_kernel(
        attend,
        like((LANES + 8, LANES), bf16),
        lengths,
        swap(heads, "kv_0"),
        key_cache.reshape(rows, columns, LANES),
        value_cache.reshape(rows, columns, LANES),
        smem=(0,),
        scratch=(
            pltpu.VMEM((LANES, columns), f32),
            pltpu.VMEM((LANES, columns), bf16),
            pltpu.VMEM((3, LANES, LANES), f32),
        ),
        vmem_limit=32 << 20,
    )
    parts = in_kernel(join, like((planes, LANES + 8, LANES), bf16), *rotations(part, "kv_1"))
    sums = in_kernel(
        finish_heads,
        sums_like,
        swap(parts, "kv_0"),
        lam_heads.reshape(1, shard_heads),
        head_gain.reshape(1, LANES),
        w_output,
    )
    sums = swap(sums, "tp")
    second, *units = in_kernel(
        last_units,
        units_like,
        sums,
        first,
        last_gain.reshape(1, LANES),
        last_gate,
        last_up,
    )
    return in_kernel(finish, like((ROWS, ROWS), bf16), hidden_sums(units, last_down), second)


def solution(mesh):
    finer = Mesh(mesh.devices.reshape(8, 4, mesh.shape["tp"]), ("kv_0", "kv_1", "tp"))
    return jax.shard_map(
        on_device,
        mesh=finer,
        in_specs=(
            P(None, KV_TP),
            P(KV),
            P(KV, "tp"),
            P(KV, "tp"),
            P("tp", KV),
            P(KV),
            P(KV, "tp"),
            P(KV, "tp"),
            P(KV, "tp"),
            P("tp", KV),
            P("tp"),
            P(),
            P(None, KV, "tp", None),
            P(None, KV, "tp", None),
            P(),
            P(KV),
            P(KV, "tp"),
            P(KV, "tp"),
            P("tp", KV),
        ),
        out_specs=P(None, KV_TP),
        check_vma=False,
    )
```
